1024 devices in a mesh: ep: 32 (over z, core), tp: 32 (over y, x).
Axes of the slice: x: 4, y: 8, z: 16, core: 2. Of those that a mesh axis runs over, the one named last changes fastest.
Arguments:
- tokens: bfloat16 [2048, 4096], P('ep', 'tp'), may hold values from -600 to 600
- in_gain: float32 [4096], P('tp'), may hold values from 0.1 to 1.9
- out_gain: float32 [4096], P('tp'), may hold values from 0.1 to 1.9
- routes: int32 [2048, 4], replicated, may hold values from 0 to 127, as said below
- route_weights: float32 [2048, 4], replicated, may hold values from 0.05 to 1
- w_gate: bfloat16 [128, 4096, 1024], P('ep', 'tp'), may hold values from -0.09375 to 0.09375
- w_up: bfloat16 [128, 4096, 1024], P('ep', 'tp'), may hold values from -0.09375 to 0.09375
- w_down: bfloat16 [128, 1024, 4096], P('ep', None, 'tp'), may hold values from -0.375 to 0.375
Outputs:
- result: bfloat16 [2048, 4096], P('ep', 'tp')
The draws below stay inside these ranges and needn't reach their ends.
Inputs may be any that keep to these rules, and one draw needn't show every extreme that they name: `routes`: each row names 4 different experts, all in one group of 8 consecutive numbers. In the rows of one index of ep (aligned blocks of 64 rows) no expert is named by more than 4 rows, and some expert by exactly 4.
All inputs are finite; a program needn't handle non-finite values.
Results may differ from the reference program's by a relative error of at most 0.025.
Values may be sent and summed in bfloat16 or wider, within the bound.
No kernel may reach another device: no remote copies, remote signals or barrier semaphores. Data moves between devices by JAX's collectives and lax.ppermute only.
A program may use at most 32 MiB of HBM per device.

```python
import math
import jax
import jax.numpy as jnp
from jax import lax

D = 4096
FF = 1024
EXP_DEV = 4
GROUP_SIZE = 8
TOP = 4
TOK_DEV = 64
SPECIALIST_COUNT = 128
GROUPS = 16
TOKENS = 2048
CAP = 4
N_EP = 32
N_TP = 32


def column_scale(key):
    columns = jnp.arange(D, dtype=jnp.float32) / D
    return jnp.exp(math.log(3.0) * columns + math.log(2.0) * jax.random.uniform(key, (D,), jnp.float32))


def draw_tokens(key, part):
    key_base, key_rows, key_cols = jax.random.split(jax.random.fold_in(key, 3), 3)
    base = jnp.clip(jax.random.normal(key_base, (TOKENS, D), jnp.float32), -6.0, 6.0)
    row_scale = jnp.exp(math.log(10.0) * jax.random.uniform(key_rows, (TOKENS, 1), jnp.float32))
    return (base * column_scale(key_cols) * row_scale).astype(jnp.bfloat16)


def draw_w_down(key, part):
    key_base, key_cols = jax.random.split(jax.random.fold_in(key, 5))
    base = jnp.clip(jax.random.normal(key_base, (SPECIALIST_COUNT, FF, D), jnp.float32), -6.0, 6.0)
    return (base * column_scale(key_cols) * FF ** (-0.5) / 3.0).astype(jnp.bfloat16)


def draw_routes(key, part):
    blocks = TOKENS // TOK_DEV
    key_rank, key_rows = jax.random.split(jax.random.fold_in(key, 7))
    ranking = jax.random.permutation(key_rank, SPECIALIST_COUNT).astype(jnp.int32)
    preferred_specialists = 12 * SPECIALIST_COUNT // (ranking + 1)
    numbers = jnp.arange(SPECIALIST_COUNT, dtype=jnp.int32)
    specialist_holders = numbers // EXP_DEV
    inside = jnp.arange(GROUP_SIZE, dtype=jnp.int32)
    group_ids = jnp.arange(GROUPS, dtype=jnp.int32)
    noise = jax.random.randint(key_rows, (blocks, TOK_DEV, SPECIALIST_COUNT), 0, 4 * SPECIALIST_COUNT, dtype=jnp.int32)

    def one_block(block, noise_rows):

        def step(counts, inputs):
            present_sequence_entry, jitter_for_entry = inputs
            destination_specialist = jnp.where(present_sequence_entry == 0, (block + blocks - 1) % blocks, (block + blocks // 2) % blocks)
            logit_offset = jnp.where((present_sequence_entry < 2) & (specialist_holders == destination_specialist), 64 * SPECIALIST_COUNT, 0).astype(jnp.int32)
            gating_logit = preferred_specialists + jitter_for_entry + logit_offset
            is_free = counts < CAP
            masked = jnp.where(is_free, gating_logit, -1).reshape(GROUPS, GROUP_SIZE)
            enough = jnp.sum(is_free.reshape(GROUPS, GROUP_SIZE).astype(jnp.int32), axis=1) >= TOP
            group_key = jnp.where(enough, jnp.max(masked, axis=1), -2) * GROUPS + group_ids
            chosen = jnp.argmax(group_key).astype(jnp.int32)
            within = lax.dynamic_index_in_dim(masked, chosen, 0, keepdims=False)
            best = lax.top_k(within * GROUP_SIZE + inside, TOP)[1].astype(jnp.int32)
            picked = chosen * GROUP_SIZE + best
            counts = counts + jnp.sum((picked[:, None] == numbers[None, :]).astype(jnp.int32), axis=0)
            return (counts, picked)
        row_ids = jnp.arange(TOK_DEV, dtype=jnp.int32)
        return lax.scan(step, jnp.zeros((SPECIALIST_COUNT,), jnp.int32), (row_ids, noise_rows))[1]
    picked_all = jax.vmap(one_block)(jnp.arange(blocks, dtype=jnp.int32), noise)
    return picked_all.reshape(TOKENS, TOP).astype(jnp.int32)


def block_scale(key, dims, cuts, smallest, top_value):
    factor_of, own = 1.0, jax.random.fold_in(key, 6)
    for dim, blocks in cuts:
        draws = jnp.exp(jax.random.uniform(jax.random.fold_in(own, dim), (blocks,), jnp.float32, smallest / len(cuts), top_value / len(cuts)))
        factor_of = factor_of * jnp.repeat(draws, dims[dim] // blocks).reshape([-1 if axis == dim else 1 for axis in range(len(dims))])
    return factor_of


def normal_values(stream_key, shape, width, limit, shards=(), kind=jnp.bfloat16):
    drawn = width * jax.random.normal(stream_key, shape, jnp.float32)
    if shards:
        drawn = drawn * block_scale(stream_key, shape, shards, -0.22, 0.18)
    return jnp.clip(drawn, -limit, limit).astype(kind)


def setup_inputs(seed: int = 0) -> dict:
    arg_keys = jax.random.split(jax.random.key(seed), 9)
    tokens = draw_tokens(jax.random.fold_in(arg_keys[8], 71), 0)
    in_gain = jnp.clip(1.0 + 0.18 * jax.random.normal(arg_keys[1], (D,), jnp.float32), 0.1, 1.9)
    out_gain = jnp.clip(1.0 + 0.18 * jax.random.normal(arg_keys[2], (D,), jnp.float32), 0.1, 1.9)
    routes = draw_routes(jax.random.fold_in(arg_keys[8], 71), 0)
    route_weights = jnp.clip(jax.random.uniform(arg_keys[4], (TOKENS, TOP), jnp.float32, 0.05, 1.0), 0.05, 1.0)
    w_gate = normal_values(arg_keys[5], (SPECIALIST_COUNT, D, FF), D ** -0.5, 0.09375, ((0, 32), (1, 32)))
    w_up = normal_values(arg_keys[6], (SPECIALIST_COUNT, D, FF), D ** -0.5, 0.09375, ((0, 32), (1, 32)))
    w_down = draw_w_down(jax.random.fold_in(arg_keys[8], 71), 0)
    return dict(tokens=tokens, in_gain=in_gain, out_gain=out_gain, routes=routes, route_weights=route_weights, w_gate=w_gate, w_up=w_up, w_down=w_down)


EPS = 1e-06

def reference(tokens, in_gain, out_gain, routes, route_weights, w_gate, w_up, w_down):
    values = tokens.astype(jnp.float32)
    normed = (values * lax.rsqrt(lax.optimization_barrier(jnp.mean(values * values, axis=1, keepdims=True)) + EPS) * in_gain).astype(jnp.bfloat16)
    local_width = D // N_TP
    slot_limit = N_EP * CAP

    def block_sum(slot_rows, weights):
        stacked = weights.astype(jnp.float32).reshape(N_TP, local_width, FF)
        parts = jnp.einsum('rjd,jdf->jrf', slot_rows, stacked).astype(jnp.bfloat16)
        parts = lax.optimization_barrier(parts)
        return lax.optimization_barrier(jnp.sum(parts.astype(jnp.float32), axis=0))

    def one_expert(combined, expert):
        matches = routes == expert
        weight = lax.optimization_barrier(jnp.sum(jnp.where(matches, route_weights, 0.0), axis=1))
        chosen = jnp.any(matches, axis=1)
        picked = jnp.nonzero(chosen, size=slot_limit, fill_value=0)[0].astype(jnp.int32)
        is_live = jnp.arange(slot_limit, dtype=jnp.int32) < jnp.sum(chosen.astype(jnp.int32))
        slot_rows = normed[picked].astype(jnp.float32).reshape(slot_limit, N_TP, local_width)
        gate_sum = block_sum(slot_rows, w_gate[expert])
        up_sum = block_sum(slot_rows, w_up[expert])
        active = (jax.nn.silu(gate_sum) * up_sum).astype(jnp.bfloat16)
        results = jnp.dot(active, w_down[expert], preferred_element_type=jnp.float32).astype(jnp.bfloat16)
        scale = jnp.where(is_live, weight[picked], 0.0)
        combined = combined.at[picked].add(scale[:, None] * results.astype(jnp.float32))
        return (combined, None)
    start = jnp.zeros((TOKENS, D), jnp.float32)
    combined, unused = lax.scan(one_expert, start, jnp.arange(SPECIALIST_COUNT, dtype=jnp.int32))
    squares = lax.optimization_barrier(jnp.mean(combined * combined, axis=1, keepdims=True))
    return (combined * lax.rsqrt(squares + EPS) * out_gain).astype(jnp.bfloat16)
```

```python
import jax
import jax.numpy as jnp
from jax import lax
from jax.experimental import pallas as pl
from jax.experimental.pallas import tpu as pltpu
from jax.sharding import Mesh, PartitionSpec as P

EPS = 1e-06
BF, F32 = jnp.bfloat16, jnp.float32
LANES = 128
HALF = 64
CAP = 4
GROUP = 8
PARAMS = pltpu.CompilerParams(vmem_limit_bytes=16 * 1024 * 1024)


def iota(shape, dim):
    return lax.broadcasted_iota(jnp.int32, shape, dim)


def ones_where(mask, dtype=BF):
    return jnp.where(mask, 1.0, 0.0).astype(dtype)


def earlier():
    s, t = iota((LANES, LANES), 0), iota((LANES, LANES), 1)
    return ones_where((s < t) & ((s >> 6) == (t >> 6)))


def dot(a, b):
    return jnp.dot(a, b, preferred_element_type=F32)


def dot_rows(a, b):
    return lax.dot_general(a, b, (((0,), (0,)), ((), ())), preferred_element_type=F32)


def call(kernel, outs, *args, name):
    single = not isinstance(outs, (list, tuple))
    return pl.pallas_call(
        kernel,
        out_shape=outs,
        in_specs=[pl.BlockSpec(memory_space=pltpu.VMEM)] * len(args),
        out_specs=pl.BlockSpec(memory_space=pltpu.VMEM)
        if single
        else [pl.BlockSpec(memory_space=pltpu.VMEM)] * len(outs),
        compiler_params=PARAMS,
        name=name,
    )(*args)


def shape(dims, dtype):
    return jax.ShapeDtypeStruct(dims, dtype)


def dispatch_kernel(routes_ref, tok_ref, out_ref, place_ref):
    z, c = lax.axis_index("z"), lax.axis_index("c")
    group = routes_ref[z, 0:1, :] >> 3
    chips = routes_ref.shape[0]
    member = iota((chips, LANES), 0) == group
    rank = dot(ones_where(member), earlier())
    rank = jnp.sum(jnp.where(member, rank, 0.0), axis=0, keepdims=True).astype(jnp.int32)
    mine = (iota((1, LANES), 1) >> 6) == c
    row = jnp.where(mine, group * GROUP + rank, -1)
    place = ones_where(iota((LANES, LANES), 0) == row)
    place_ref[...] = place
    tok = tok_ref[...]
    out_ref[...] = dot(place, jnp.concatenate([tok, tok], axis=0)).astype(BF)


def table_kernel(routes_ref, weights_ref, sel_ref, scale_ref):
    z, c, x = lax.axis_index("z"), lax.axis_index("c"), lax.axis_index("x")
    chips = routes_ref.shape[0]
    ids = [routes_ref[:, k, :] for k in range(CAP)]
    before = earlier()
    base = z * GROUP

    def named(expert):
        hit = ids[0] == expert
        for k in range(1, CAP):
            hit = hit | (ids[k] == expert)
        return jnp.where(hit, 1.0, 0.0)

    rows = [named(base + e) for e in range(GROUP)]
    hits = jnp.concatenate(rows, axis=0)
    anyone = rows[0]
    for e in range(1, GROUP):
        anyone = jnp.maximum(anyone, rows[e])
    rank = dot(hits.astype(BF), before)
    spot = dot(anyone.astype(BF), before) + (iota((chips, LANES), 0) * GROUP).astype(F32)
    spots = jnp.concatenate([spot] * GROUP, axis=0)
    block = iota((LANES, LANES), 1) >> 6
    lane = iota((LANES, LANES), 1).astype(F32)
    live = (hits > 0.0) & (block == c)
    for q in range(CAP):
        at = jnp.sum(jnp.where(live & (rank == q), spots + 1.0, 0.0), axis=1, keepdims=True) - 1.0
        sel_ref[q] = ones_where(lane == at)
    own = base + c * CAP + x
    own_hit = named(own)
    own_rank = dot(own_hit.astype(BF), before)
    weight = jnp.zeros((chips, LANES), F32)
    for k in range(CAP):
        weight = weight + jnp.where(ids[k] == own, weights_ref[:, k, :], 0.0)
    small_block = iota((chips, LANES), 1) >> 6
    for core in range(2):
        for q in range(CAP):
            at = (own_hit > 0.0) & (own_rank == q) & (small_block == core)
            value = jnp.sum(jnp.where(at, weight, 0.0), axis=1, keepdims=True)
            start = (core * CAP + q) * chips
            scale_ref[start : start + chips, :] = jnp.broadcast_to(value, (chips, LANES))


def select_kernel(recv_ref, sel_ref, gain_ref, out_ref):
    recv = recv_ref[...]
    for q in range(CAP):
        picked = dot(sel_ref[q], recv).astype(BF)
        for e in range(GROUP):
            out_ref[e, q * 16 : (q + 1) * 16, :] = picked[e * 16 : (e + 1) * 16]
    gain = gain_ref[...]
    high = gain.astype(BF)
    rest = gain - high.astype(F32)
    middle = rest.astype(BF)
    low = (rest - middle.astype(F32)).astype(BF)
    row = iota((8, LANES), 0)
    tail = jnp.where(
        row == 0,
        high.astype(F32),
        jnp.where(row == 1, middle.astype(F32), jnp.where(row == 2, low.astype(F32), 0.0)),
    ).astype(BF)
    for e in range(GROUP):
        out_ref[e, 64:72, :] = tail


def gate_up_kernel(rows_ref, gate_ref, up_ref, out_ref):
    squares = jnp.zeros((LANES, 1), F32)
    parts = []
    for x in range(4):
        raw = jnp.concatenate([rows_ref[x, 0:64, :], rows_ref[4 + x, 0:64, :]], axis=0).astype(F32)
        tail = rows_ref[x, 64:72, :].astype(F32)
        gain = tail[0:1] + tail[1:2] + tail[2:3]
        squares = squares + jnp.sum(raw * raw, axis=1, keepdims=True)
        parts.append((raw * gain).astype(BF))
    lhs = jnp.concatenate(parts, axis=1)
    hidden = gate_ref.shape[1]
    out_ref[:, 0:hidden] = dot(lhs, gate_ref[...]).astype(BF)
    out_ref[:, hidden : 2 * hidden] = dot(lhs, up_ref[...]).astype(BF)
    high = squares.astype(BF).astype(F32)
    lane = iota((LANES, LANES), 1)
    out_ref[:, 2 * hidden :] = jnp.where(lane < HALF, high, squares - high).astype(BF)


def act_kernel(width, parts_ref, out_ref):
    total = parts_ref[0].astype(F32)
    for y in range(1, parts_ref.shape[0]):
        total = total + parts_ref[y].astype(F32)
    hidden = out_ref.shape[2]
    squares = total[:, 2 * hidden : 2 * hidden + 1] + total[:, 2 * hidden + HALF : 2 * hidden + HALF + 1]
    scale = lax.rsqrt(squares / width + EPS)
    gate = total[:, 0:hidden] * scale
    up = total[:, hidden : 2 * hidden] * scale
    act = (gate / (1.0 + jnp.exp(-gate)) * up).astype(BF)
    for y in range(out_ref.shape[0]):
        out_ref[y] = act


def down_kernel(act_ref, down_ref, scale_ref, out_ref):
    act = act_ref[...]
    scale = scale_ref[...]
    for x in range(4):
        out = (dot(act, down_ref[x]) * scale).astype(BF)
        out_ref[x] = out[0:64]
        out_ref[4 + x] = out[64:128]


def combine_kernel(parts_ref, sel_ref, out_ref):
    total = jnp.zeros((LANES, LANES), F32)
    for q in range(CAP):
        rows = jnp.concatenate(
            [parts_ref[e, q * 16 : (q + 1) * 16, :] for e in range(GROUP)], axis=0
        )
        total = total + dot_rows(sel_ref[q], rows)
    out_ref[...] = total.astype(BF)


def place_kernel(ret_ref, place_ref, comb_ref, squares_ref):
    full = dot_rows(place_ref[...], ret_ref[...])
    comb_ref[...] = full[0:HALF] + full[HALF:LANES]
    squares = jnp.sum(full * full, axis=1, keepdims=True)
    flat = jnp.transpose(jnp.broadcast_to(squares, (LANES, LANES)))[0:1, :]
    for i in range(squares_ref.shape[0]):
        squares_ref[i] = flat


def norm_kernel(width, squares_ref, comb_ref, gain_ref, out_ref):
    total = squares_ref[0]
    for i in range(1, squares_ref.shape[0]):
        total = total + squares_ref[i]
    column = jnp.transpose(jnp.broadcast_to(total, (LANES, LANES)))
    column = column[0:HALF] + column[HALF:LANES]
    out_ref[...] = (comb_ref[...] * lax.rsqrt(column / width + EPS) * gain_ref[...]).astype(BF)


def exchange(value, axes):
    return lax.all_to_all(value, axes, 0, 0, tiled=True)


def on_device(tokens, in_gain, out_gain, routes, route_weights, w_gate, w_up, w_down):
    chips, ys, xs = lax.axis_size("z"), lax.axis_size("y"), lax.axis_size("x")
    local = tokens.shape[1]
    width = float(local * ys * xs)
    hidden = w_gate.shape[2]
    routes = jnp.transpose(routes.reshape(chips, LANES, CAP), (0, 2, 1))
    weights = jnp.transpose(route_weights.reshape(chips, LANES, CAP), (0, 2, 1))

    gate_rows = exchange(w_gate, "x").reshape(xs * local, hidden)
    up_rows = exchange(w_up, "x").reshape(xs * local, hidden)
    outgoing, place = call(
        dispatch_kernel,
        [shape((LANES, LANES), BF), shape((LANES, LANES), BF)],
        routes,
        tokens,
        name="dispatch",
    )
    sel, scale = call(
        table_kernel,
        [shape((CAP, LANES, LANES), BF), shape((LANES, LANES), F32)],
        routes,
        weights,
        name="tables",
    )
    arrived = exchange(outgoing.reshape(chips, GROUP, local), "z").reshape(LANES, local)
    slots = call(
        select_kernel,
        shape((GROUP, 72, LANES), BF),
        arrived,
        sel,
        in_gain.reshape(1, local),
        name="select",
    )
    slots = exchange(slots, ("c", "x"))
    parts = call(
        gate_up_kernel,
        shape((LANES, 2 * hidden + LANES), BF),
        slots,
        gate_rows,
        up_rows,
        name="gate_up",
    )
    down_rows = exchange(w_down, "x")
    parts = exchange(parts.reshape(ys, LANES // ys, 2 * hidden + LANES), "y")
    act = call(
        lambda *refs: act_kernel(width, *refs),
        shape((ys, LANES // ys, hidden), BF),
        parts,
        name="act",
    )
    act = exchange(act, "y").reshape(LANES, hidden)
    answers = call(
        down_kernel, shape((GROUP, 64, LANES), BF), act, down_rows, scale, name="down"
    )
    answers = exchange(answers, ("c", "x"))
    mixed = call(combine_kernel, shape((LANES, local), BF), answers, sel, name="combine")
    returned = exchange(mixed.reshape(chips, GROUP, local), "z").reshape(LANES, local)
    combined, squares = call(
        place_kernel,
        [shape((HALF, local), F32), shape((ys * xs, 1, LANES), F32)],
        returned,
        place,
        name="place",
    )
    squares = exchange(squares, ("y", "x"))
    return call(
        lambda *refs: norm_kernel(width, *refs),
        shape((HALF, local), BF),
        squares,
        combined,
        out_gain.reshape(1, local),
        name="norm",
    )


def solution(mesh):
    fine = Mesh(
        mesh.devices.reshape(mesh.shape["ep"] // 2, 2, mesh.shape["tp"] // 4, 4),
        ("z", "c", "y", "x"),
    )
    ep, tp = ("z", "c"), ("y", "x")
    placed = (
        P(ep, tp),
        P(tp),
        P(tp),
        P(),
        P(),
        P(ep, tp, None),
        P(ep, tp, None),
        P(ep, None, tp),
    )
    return jax.shard_map(
        on_device, mesh=fine, in_specs=placed, out_specs=P(ep, tp), check_vma=False
    )
```

```python
import jax
import jax.numpy as jnp
from jax import lax
from jax.experimental import pallas as pl
from jax.experimental.pallas import tpu as pltpu
from jax.sharding import Mesh, PartitionSpec as P

EPS = 1e-06
BF, F32 = jnp.bfloat16, jnp.float32
LANES = 128
HALF = 64
CAP = 4
GROUP = 8
PARAMS = pltpu.CompilerParams(vmem_limit_bytes=16 * 1024 * 1024)


def iota(shape, dim):
    return lax.broadcasted_iota(jnp.int32, shape, dim)


def ones_where(mask, dtype=BF):
    return jnp.where(mask, 1.0, 0.0).astype(dtype)


def earlier():
    s, t = iota((LANES, LANES), 0), iota((LANES, LANES), 1)
    return ones_where((s < t) & ((s >> 6) == (t >> 6)))


def dot(a, b):
    return jnp.dot(a, b, preferred_element_type=F32)


def dot_rows(a, b):
    return lax.dot_general(a, b, (((0,), (0,)), ((), ())), preferred_element_type=F32)


def call(kernel, outs, *args):
    single = not isinstance(outs, (list, tuple))
    return pl.pallas_call(
        kernel,
        out_shape=outs,
        in_specs=[pl.BlockSpec(memory_space=pltpu.VMEM)] * len(args),
        out_specs=pl.BlockSpec(memory_space=pltpu.VMEM)
        if single
        else [pl.BlockSpec(memory_space=pltpu.VMEM)] * len(outs),
        compiler_params=PARAMS,
    )(*args)


def shape(dims, dtype):
    return jax.ShapeDtypeStruct(dims, dtype)


def dispatch_kernel(routes_ref, tok_ref, out_ref, place_ref):
    z, c = lax.axis_index("z"), lax.axis_index("c")
    group = routes_ref[z, 0:1, :] >> 3
    chips = routes_ref.shape[0]
    member = iota((chips, LANES), 0) == group
    rank = dot(ones_where(member), earlier())
    rank = jnp.sum(jnp.where(member, rank, 0.0), axis=0, keepdims=True).astype(jnp.int32)
    mine = (iota((1, LANES), 1) >> 6) == c
    row = jnp.where(mine, group * GROUP + rank, -1)
    place = ones_where(iota((LANES, LANES), 0) == row)
    place_ref[...] = place
    tok = tok_ref[...]
    out_ref[...] = dot(place, jnp.concatenate([tok, tok], axis=0)).astype(BF)


def named(ids, expert):
    hit = ids[0] == expert
    for k in range(1, CAP):
        hit = hit | (ids[k] == expert)
    return jnp.where(hit, 1.0, 0.0)


def table_kernel(routes_ref, sel_ref):
    z, c = lax.axis_index("z"), lax.axis_index("c")
    chips = routes_ref.shape[0]
    ids = [routes_ref[:, k, :] for k in range(CAP)]
    before = earlier()
    rows = [named(ids, z * GROUP + e) for e in range(GROUP)]
    hits = jnp.concatenate(rows, axis=0)
    anyone = rows[0]
    for e in range(1, GROUP):
        anyone = jnp.maximum(anyone, rows[e])
    rank = dot(hits.astype(BF), before)
    spot = dot(anyone.astype(BF), before) + (iota((chips, LANES), 0) * GROUP).astype(F32)
    spots = jnp.concatenate([spot] * GROUP, axis=0)
    lane = iota((LANES, LANES), 1).astype(F32)
    live = (hits > 0.0) & ((iota((LANES, LANES), 1) >> 6) == c)
    for q in range(CAP):
        at = jnp.sum(jnp.where(live & (rank == q), spots + 1.0, 0.0), axis=1, keepdims=True) - 1.0
        sel_ref[q] = ones_where(lane == at)


def scale_kernel(routes_ref, weights_ref, scale_ref):
    z, c, x = lax.axis_index("z"), lax.axis_index("c"), lax.axis_index("x")
    chips = routes_ref.shape[0]
    ids = [routes_ref[:, k, :] for k in range(CAP)]
    own = z * GROUP + c * CAP + x
    hit = named(ids, own)
    rank = dot(hit.astype(BF), earlier())
    weight = jnp.zeros((chips, LANES), F32)
    for k in range(CAP):
        weight = weight + jnp.where(ids[k] == own, weights_ref[:, k, :], 0.0)
    block = iota((chips, LANES), 1) >> 6
    for core in range(2):
        for q in range(CAP):
            at = (hit > 0.0) & (rank == q) & (block == core)
            value = jnp.sum(jnp.where(at, weight, 0.0), axis=1, keepdims=True)
            start = (core * CAP + q) * chips
            scale_ref[start : start + chips, :] = jnp.broadcast_to(value, (chips, LANES))


def deal_kernel(*refs):
    x = lax.axis_index("x")
    n = lax.axis_size("x")
    sources, outs, sems = refs[: len(refs) - 1 - n], refs[len(refs) - 1 - n : -1], refs[-1]
    copies = []
    for d in range(n):
        for i, source in enumerate(sources):
            copies.append(
                pltpu.make_async_copy(
                    source.at[lax.rem(x + d, n)], outs[d].at[i], sems.at[d * len(sources) + i]
                )
            )
    for copy in copies:
        copy.start()
    for copy in copies:
        copy.wait()


def deal(arrays):
    n = arrays[0].shape[0]
    one = shape((len(arrays), *arrays[0].shape[1:]), BF)
    return pl.pallas_call(
        deal_kernel,
        out_shape=[one] * n,
        in_specs=[pl.BlockSpec(memory_space=pl.ANY)] * len(arrays),
        out_specs=[pl.BlockSpec(memory_space=pltpu.VMEM)] * n,
        scratch_shapes=[pltpu.SemaphoreType.DMA((n * len(arrays),))],
        compiler_params=PARAMS,
    )(*arrays)


def passed(pieces, axis):
    n = lax.axis_size(axis)
    moved = [pieces[0]]
    for d in range(1, n):
        moved.append(lax.ppermute(pieces[d], axis, [(i, (i + d) % n) for i in range(n)]))
    return moved


def select_kernel(recv_ref, sel_ref, gain_ref, out_ref):
    recv = recv_ref[...]
    for q in range(CAP):
        picked = dot(sel_ref[q], recv).astype(BF)
        for e in range(GROUP):
            out_ref[e, q * 16 : (q + 1) * 16, :] = picked[e * 16 : (e + 1) * 16]
    gain = gain_ref[...]
    high = gain.astype(BF)
    rest = gain - high.astype(F32)
    middle = rest.astype(BF)
    low = (rest - middle.astype(F32)).astype(BF)
    row = iota((8, LANES), 0)
    tail = jnp.where(
        row == 0,
        high.astype(F32),
        jnp.where(row == 1, middle.astype(F32), jnp.where(row == 2, low.astype(F32), 0.0)),
    ).astype(BF)
    for e in range(GROUP):
        out_ref[e, 64:72, :] = tail


def gate_up_kernel(rows_ref, *refs):
    *weights, out_ref = refs
    n = len(weights)
    x = lax.axis_index("x")
    squares = jnp.zeros((LANES, 1), F32)
    hidden = weights[0].shape[2]
    gate = jnp.zeros((LANES, hidden), F32)
    up = jnp.zeros((LANES, hidden), F32)
    for d in range(n):
        at = lax.rem(x - d + n, n)
        raw = jnp.concatenate([rows_ref[at, 0:64, :], rows_ref[n + at, 0:64, :]], axis=0)
        raw = raw.astype(F32)
        tail = rows_ref[at, 64:72, :].astype(F32)
        gain = tail[0:1] + tail[1:2] + tail[2:3]
        squares = squares + jnp.sum(raw * raw, axis=1, keepdims=True)
        lhs = (raw * gain).astype(BF)
        gate = gate + dot(lhs, weights[d][0])
        up = up + dot(lhs, weights[d][1])
    out_ref[:, 0:hidden] = gate.astype(BF)
    out_ref[:, hidden : 2 * hidden] = up.astype(BF)
    high = squares.astype(BF).astype(F32)
    lane = iota((LANES, LANES), 1)
    out_ref[:, 2 * hidden :] = jnp.where(lane < HALF, high, squares - high).astype(BF)


def act_kernel(width, parts_ref, out_ref):
    total = parts_ref[0].astype(F32)
    for y in range(1, parts_ref.shape[0]):
        total = total + parts_ref[y].astype(F32)
    hidden = out_ref.shape[2]
    squares = total[:, 2 * hidden : 2 * hidden + 1] + total[:, 2 * hidden + HALF : 2 * hidden + HALF + 1]
    scale = lax.rsqrt(squares / width + EPS)
    gate = total[:, 0:hidden] * scale
    up = total[:, hidden : 2 * hidden] * scale
    act = (gate / (1.0 + jnp.exp(-gate)) * up).astype(BF)
    for y in range(out_ref.shape[0]):
        out_ref[y] = act


def down_kernel(act_ref, scale_ref, *refs):
    *weights, out_ref = refs
    n = len(weights)
    x = lax.axis_index("x")
    act = act_ref[...]
    scale = scale_ref[...]
    for d in range(n):
        at = lax.rem(x - d + n, n)
        out = (dot(act, weights[d][0]) * scale).astype(BF)
        out_ref[at] = out[0:64]
        out_ref[n + at] = out[64:128]


def combine_kernel(parts_ref, sel_ref, out_ref):
    total = jnp.zeros((LANES, LANES), F32)
    for q in range(CAP):
        rows = jnp.concatenate(
            [parts_ref[e, q * 16 : (q + 1) * 16, :] for e in range(GROUP)], axis=0
        )
        total = total + dot_rows(sel_ref[q], rows)
    out_ref[...] = total.astype(BF)


def place_kernel(ret_ref, place_ref, comb_ref, squares_ref):
    full = dot_rows(place_ref[...], ret_ref[...])
    comb_ref[...] = full[0:HALF] + full[HALF:LANES]
    squares = jnp.sum(full * full, axis=1, keepdims=True)
    flat = jnp.transpose(jnp.broadcast_to(squares, (LANES, LANES)))[0:1, :]
    for i in range(squares_ref.shape[0]):
        squares_ref[i] = flat


def norm_kernel(width, squares_ref, comb_ref, gain_ref, out_ref):
    total = squares_ref[0]
    for i in range(1, squares_ref.shape[0]):
        total = total + squares_ref[i]
    column = jnp.transpose(jnp.broadcast_to(total, (LANES, LANES)))
    column = column[0:HALF] + column[HALF:LANES]
    out_ref[...] = (comb_ref[...] * lax.rsqrt(column / width + EPS) * gain_ref[...]).astype(BF)


def exchange(value, axes):
    return lax.all_to_all(value, axes, 0, 0, tiled=True)


def on_device(tokens, in_gain, out_gain, routes, route_weights, w_gate, w_up, w_down):
    chips, ys, xs = lax.axis_size("z"), lax.axis_size("y"), lax.axis_size("x")
    local = tokens.shape[1]
    width = float(local * ys * xs)
    hidden = w_gate.shape[2]
    routes = jnp.transpose(routes.reshape(chips, LANES, CAP), (0, 2, 1))
    weights = jnp.transpose(route_weights.reshape(chips, LANES, CAP), (0, 2, 1))

    gate_up = passed(deal([w_gate, w_up]), "x")
    outgoing, place = call(
        dispatch_kernel, [shape((LANES, LANES), BF), shape((LANES, LANES), BF)], routes, tokens
    )
    sel = call(table_kernel, shape((CAP, LANES, LANES), BF), routes)
    scale = call(scale_kernel, shape((LANES, LANES), F32), routes, weights)
    arrived = exchange(outgoing.reshape(chips, GROUP, local), "z").reshape(LANES, local)
    slots = call(
        select_kernel, shape((GROUP, 72, LANES), BF), arrived, sel, in_gain.reshape(1, local)
    )
    slots = exchange(slots, ("c", "x"))
    parts = call(gate_up_kernel, shape((LANES, 2 * hidden + LANES), BF), slots, *gate_up)
    down_rows = passed(deal([w_down]), "x")
    parts = exchange(parts.reshape(ys, LANES // ys, 2 * hidden + LANES), "y")
    act = call(lambda *refs: act_kernel(width, *refs), shape((ys, LANES // ys, hidden), BF), parts)
    act = exchange(act, "y").reshape(LANES, hidden)
    answers = call(down_kernel, shape((GROUP, 64, LANES), BF), act, scale, *down_rows)
    answers = exchange(answers, ("c", "x"))
    mixed = call(combine_kernel, shape((LANES, local), BF), answers, sel)
    returned = exchange(mixed.reshape(chips, GROUP, local), "z").reshape(LANES, local)
    combined, squares = call(
        place_kernel, [shape((HALF, local), F32), shape((ys * xs, 1, LANES), F32)], returned, place
    )
    squares = exchange(squares, ("y", "x"))
    return call(
        lambda *refs: norm_kernel(width, *refs),
        shape((HALF, local), BF),
        squares,
        combined,
        out_gain.reshape(1, local),
    )


def solution(mesh):
    fine = Mesh(
        mesh.devices.reshape(mesh.shape["ep"] // 2, 2, mesh.shape["tp"] // 4, 4),
        ("z", "c", "y", "x"),
    )
    ep, tp = ("z", "c"), ("y", "x")
    placed = (
        P(ep, tp),
        P(tp),
        P(tp),
        P(),
        P(),
        P(ep, tp, None),
        P(ep, tp, None),
        P(ep, None, tp),
    )

    return jax.shard_map(on_device, mesh=fine, in_specs=placed, out_specs=P(ep, tp), check_vma=False)
```

```python
import jax
import jax.numpy as jnp
from jax import lax
from jax.experimental import pallas as pl
from jax.experimental.pallas import tpu as pltpu
from jax.sharding import Mesh, PartitionSpec as P

EPS = 1e-06
BF, F32 = jnp.bfloat16, jnp.float32
LANES = 128
HALF = 64
CAP = 4
GROUP = 8
PIECES = 1
PARAMS = pltpu.CompilerParams(vmem_limit_bytes=16 * 1024 * 1024)
FIRST = {"z": lambda n: 13, "c": lambda n: n - 1, "y": lambda n: n // 2, "x": lambda n: n // 2}
STEP = {"z": 1, "c": 1, "y": 1, "x": 1}
REDUCE = [4, 7, 2, 5, 0, 3, 6, 1]
GATHER = [4, 7, 2, 5, 0, 3, 6, 1]
VMEM = pl.BlockSpec(memory_space=pltpu.VMEM)
HBM = pl.BlockSpec(memory_space=pltpu.HBM)


def in_hbm(value):
    return pltpu.with_memory_space_constraint(value, pltpu.HBM)


def shape(dims, dtype):
    return jax.ShapeDtypeStruct(dims, dtype)


def iota(dims, dim):
    return lax.broadcasted_iota(jnp.int32, dims, dim)


def ones_where(mask, dtype=BF):
    return jnp.where(mask, 1.0, 0.0).astype(dtype)


def earlier():
    s, t = iota((LANES, LANES), 0), iota((LANES, LANES), 1)
    return ones_where((s < t) & ((s >> 6) == (t >> 6)))


def dot(a, b):
    return jnp.dot(a, b, preferred_element_type=F32)


def dot_rows(a, b):
    return lax.dot_general(a, b, (((0,), (0,)), ((), ())), preferred_element_type=F32)


def call(kernel, outs, *args):
    single = not isinstance(outs, (list, tuple))
    return pl.pallas_call(
        kernel,
        out_shape=outs,
        in_specs=[VMEM] * len(args),
        out_specs=VMEM if single else [VMEM] * len(outs),
        compiler_params=PARAMS,
    )(*args)


def place_of(index, axis):
    n = lax.axis_size(axis)
    return lax.rem(index + n - FIRST[axis](n), n)


def named(ids, expert):
    hit = ids[0] == expert
    for k in range(1, CAP):
        hit = hit | (ids[k] == expert)
    return jnp.where(hit, 1.0, 0.0)


def slice_copies(sources, outs, shifts, sems):
    x = lax.axis_index("x")
    copies = []
    for d, out in zip(shifts, outs):
        for i, source in enumerate(sources):
            at = lax.rem(x + d, source.shape[0])
            rows = source.shape[1] // PIECES
            for k in range(PIECES):
                part = pl.ds(k * rows, rows)
                copies.append(
                    pltpu.make_async_copy(
                        source.at[at, part, :], out.at[i, part, :], sems.at[len(copies)]
                    )
                )
    return copies


def deal(arrays, shifts, kernel=None, extra=(), extra_outs=()):
    one = shape((len(arrays), *arrays[0].shape[1:]), BF)
    n, m, k = len(arrays), len(shifts), len(extra)

    def body(*refs):
        sources, small, rest = refs[:n], refs[n : n + k], refs[n + k :]
        outs, held, sems, small_sems = rest[: len(rest) - k - 2], rest[-k - 2 : -2], *rest[-2:]
        fetches = [
            pltpu.make_async_copy(small[i], held[i], small_sems.at[i]) for i in range(k)
        ]
        copies = slice_copies(sources, outs[:m], shifts, sems)
        for copy in fetches + copies:
            copy.start()
        for copy in fetches:
            copy.wait()
        if kernel is not None:
            kernel(*held, *outs[m:])
        for copy in copies:
            copy.wait()

    return pl.pallas_call(
        body,
        out_shape=[one] * m + list(extra_outs),
        in_specs=[HBM] * (n + k),
        out_specs=[VMEM] * (m + len(extra_outs)),
        scratch_shapes=[pltpu.VMEM(a.shape, a.dtype) for a in extra]
        + [pltpu.SemaphoreType.DMA((m * n * PIECES,)), pltpu.SemaphoreType.DMA((max(k, 1),))],
        compiler_params=PARAMS,
    )(*[in_hbm(a) for a in (*arrays, *extra)])


def dispatch(ids, tok_ref, out_ref, place_ref):
    z, c = lax.axis_index("z"), lax.axis_index("c")
    chips = ids[0].shape[0]
    first = jnp.sum(jnp.where(iota(ids[0].shape, 0) == z, ids[0], 0), axis=0, keepdims=True)
    group = first >> 3
    member = iota((chips, LANES), 0) == group
    rank = dot(ones_where(member), earlier())
    rank = jnp.sum(jnp.where(member, rank, 0.0), axis=0, keepdims=True).astype(jnp.int32)
    mine = (iota((1, LANES), 1) >> 6) == c
    row = jnp.where(mine, place_of(group, "z") * GROUP + rank, -1)
    place = ones_where(iota((LANES, LANES), 0) == row)
    place_ref[...] = place
    tok = tok_ref[...]
    out_ref[...] = dot(place, jnp.concatenate([tok, tok], axis=0)).astype(BF)


def select_table(ids, sel_ref):
    z, c = lax.axis_index("z"), lax.axis_index("c")
    chips = ids[0].shape[0]
    before = earlier()
    rows = [named(ids, z * GROUP + e) for e in listed(("c", "x"))]
    hits = jnp.concatenate(rows, axis=0)
    anyone = rows[0]
    for e in range(1, GROUP):
        anyone = jnp.maximum(anyone, rows[e])
    rank = dot(hits.astype(BF), before)
    start = (place_of(iota((chips, LANES), 0), "z") * GROUP).astype(F32)
    spot = dot(anyone.astype(BF), before) + start
    spots = jnp.concatenate([spot] * GROUP, axis=0)
    lane = iota((LANES, LANES), 1).astype(F32)
    live = (hits > 0.0) & ((iota((LANES, LANES), 1) >> 6) == c)
    for q in range(CAP):
        at = jnp.sum(jnp.where(live & (rank == q), spots + 1.0, 0.0), axis=1, keepdims=True) - 1.0
        sel_ref[q] = ones_where(lane == at)


def slot_scales(ids, weights_ref, scale_ref):
    z, c, x = lax.axis_index("z"), lax.axis_index("c"), lax.axis_index("x")
    chips = ids[0].shape[0]
    own = z * GROUP + c * CAP + x
    hit = named(ids, own)
    rank = dot(hit.astype(BF), earlier())
    weight = jnp.zeros((chips, LANES), F32)
    for k in range(CAP):
        weight = weight + jnp.where(ids[k] == own, weights_ref[:, k, :], 0.0)
    block = iota((chips, LANES), 1) >> 6
    for i, core in enumerate(listed(("c",))):
        for q in range(CAP):
            at = (hit > 0.0) & (rank == q) & (block == core)
            value = jnp.sum(jnp.where(at, weight, 0.0), axis=1, keepdims=True)
            start = (i * CAP + q) * chips
            scale_ref[start : start + chips, :] = jnp.broadcast_to(value, (chips, LANES))


def three_rows(gain, tail_ref):
    high = gain.astype(BF).astype(F32)
    middle = (gain - high).astype(BF).astype(F32)
    low = gain - high - middle
    row = iota((8, LANES), 0)
    tail = jnp.where(row == 0, high, jnp.where(row == 1, middle, jnp.where(row == 2, low, 0.0)))
    tail_ref[...] = tail.astype(BF)


def routing_kernel(
    routes_ref, weights_ref, tok_ref, gain_ref, last_ref,
    out_ref, place_ref, sel_ref, tail_ref, scale_ref, last_out_ref,
):
    ids = [routes_ref[:, k, :] for k in range(CAP)]
    dispatch(ids, tok_ref, out_ref, place_ref)
    select_table(ids, sel_ref)
    three_rows(gain_ref[...], tail_ref)
    slot_scales(ids, weights_ref, scale_ref)
    last_out_ref[...] = jnp.broadcast_to(last_ref[...], last_out_ref.shape)


def passed(piece, d, axis):
    n = lax.axis_size(axis)
    return lax.ppermute(piece, axis, [(i, (i + d) % n) for i in range(n)])


def mark_kernel(in_ref, out_ref):
    out_ref[...] = in_ref[...]


def select_kernel(recv_ref, sel_ref, tail_ref, out_ref):
    recv = recv_ref[...]
    for q in range(CAP):
        picked = dot(sel_ref[q], recv).astype(BF)
        for e in range(GROUP):
            out_ref[e, q * 16 : (q + 1) * 16, :] = picked[e * 16 : (e + 1) * 16]
    tail = tail_ref[...]
    for e in range(GROUP):
        out_ref[e, 64:72, :] = tail


def gate_up_kernel(rows_ref, *refs):
    *weights, out_ref = refs
    n = len(weights)
    x = lax.axis_index("x")
    squares = jnp.zeros((LANES, 1), F32)
    hidden = weights[0].shape[2]
    gate = jnp.zeros((LANES, hidden), F32)
    up = jnp.zeros((LANES, hidden), F32)
    for d in range(n):
        at = place_of(x - d + n, "x")
        raw = jnp.concatenate([rows_ref[at, 0:64, :], rows_ref[n + at, 0:64, :]], axis=0)
        raw = raw.astype(F32)
        tail = rows_ref[at, 64:72, :].astype(F32)
        gain = tail[0:1] + tail[1:2] + tail[2:3]
        squares = squares + jnp.sum(raw * raw, axis=1, keepdims=True)
        lhs = (raw * gain).astype(BF)
        gate = gate + dot(lhs, weights[d][0])
        up = up + dot(lhs, weights[d][1])
    out_ref[:, 0:hidden] = gate.astype(BF)
    out_ref[:, hidden : 2 * hidden] = up.astype(BF)
    high = squares.astype(BF).astype(F32)
    lane = iota((LANES, LANES), 1)
    out_ref[:, 2 * hidden :] = jnp.where(lane < HALF, high, squares - high).astype(BF)


def act_kernel(width, parts_ref, out_ref):
    total = parts_ref[0].astype(F32)
    for y in range(1, parts_ref.shape[0]):
        total = total + parts_ref[y].astype(F32)
    hidden = out_ref.shape[2]
    squares = total[:, 2 * hidden : 2 * hidden + 1] + total[:, 2 * hidden + HALF : 2 * hidden + HALF + 1]
    scale = lax.rsqrt(squares / width + EPS)
    gate = total[:, 0:hidden] * scale
    up = total[:, hidden : 2 * hidden] * scale
    act = (gate / (1.0 + jnp.exp(-gate)) * up).astype(BF)
    for y in range(out_ref.shape[0]):
        out_ref[y] = act


def down_kernel(act_ref, scale_ref, *refs):
    *weights, out_ref = refs
    n = len(weights)
    x = lax.axis_index("x")
    rows = act_ref.shape[0] // len(GATHER)
    at = [GATHER.index(y) * rows for y in REDUCE]
    act = jnp.concatenate([act_ref[i : i + rows, :] for i in at], axis=0)
    scale = scale_ref[...]
    for d in range(n):
        at = place_of(x - d + n, "x")
        out = (dot(act, weights[d][0]) * scale).astype(BF)
        out_ref[at] = out[0:64]
        out_ref[n + at] = out[64:128]


def combine_kernel(parts_ref, sel_ref, out_ref):
    total = jnp.zeros((LANES, LANES), F32)
    for q in range(CAP):
        rows = jnp.concatenate(
            [parts_ref[e, q * 16 : (q + 1) * 16, :] for e in range(GROUP)], axis=0
        )
        total = total + dot_rows(sel_ref[q], rows)
    out_ref[...] = total.astype(BF)


def place_kernel(ret_ref, place_ref, comb_ref, squares_ref):
    full = dot_rows(place_ref[...], ret_ref[...])
    comb_ref[...] = full[0:HALF] + full[HALF:LANES]
    squares = jnp.sum(full * full, axis=1, keepdims=True)
    flat = jnp.transpose(jnp.broadcast_to(squares, (LANES, LANES)))[0:1, :]
    for i in range(squares_ref.shape[0]):
        squares_ref[i] = flat


def norm_kernel(width, squares_ref, comb_ref, gain_ref, out_ref):
    total = squares_ref[0]
    for i in range(1, squares_ref.shape[0]):
        total = total + squares_ref[i]
    column = jnp.transpose(jnp.broadcast_to(total, (LANES, LANES)))
    column = column[0:HALF] + column[HALF:LANES]
    out_ref[...] = (comb_ref[...] * lax.rsqrt(column / width + EPS) * gain_ref[0:1, :]).astype(BF)


def listed(axes):
    order = [0]
    for axis in axes:
        n = lax.axis_size(axis)
        order = [i * n + (FIRST[axis](n) + STEP[axis] * k) % n for i in order for k in range(n)]
    return order


def exchange(value, axes, order=None):
    groups = [listed(axes) if order is None else order]
    return lax.all_to_all(value, axes, 0, 0, tiled=True, axis_index_groups=groups)


def on_device(tokens, in_gain, out_gain, routes, route_weights, w_gate, w_up, w_down):
    chips, ys, xs = lax.axis_size("z"), lax.axis_size("y"), lax.axis_size("x")
    local = tokens.shape[1]
    width = float(local * ys * xs)
    hidden = w_gate.shape[2]
    routes = jnp.transpose(routes.reshape(chips, LANES, CAP), (0, 2, 1))
    weights = jnp.transpose(route_weights.reshape(chips, LANES, CAP), (0, 2, 1))

    square = shape((LANES, LANES), BF)
    own, near, far, back, outgoing, place, sel, tail, scale, last_gain = deal(
        [w_gate, w_up],
        [0, 1, 2, 3],
        routing_kernel,
        (routes, weights, tokens, in_gain.reshape(1, local), out_gain.reshape(1, local)),
        (
            square,
            square,
            shape((CAP, LANES, LANES), BF),
            shape((8, LANES), BF),
            shape((LANES, LANES), F32),
            shape((8, LANES), F32),
        ),
    )
    gate_up = [own, passed(near, 1, "x"), passed(far, 2, "x"), passed(back, 3, "x")]
    own, near, far, back = deal([w_down], [0, 1, 2, 3])
    down = [own, passed(near, 1, "x"), passed(far, 2, "x"), passed(back, 3, "x")]
    arrived = exchange(outgoing.reshape(chips, GROUP, local), ("z",))
    slots = call(
        select_kernel, shape((GROUP, 72, LANES), BF), arrived.reshape(LANES, local), sel, tail
    )
    slots = exchange(slots, ("c", "x"))
    parts = call(gate_up_kernel, shape((LANES, 2 * hidden + LANES), BF), slots, *gate_up)
    last_gain = call(mark_kernel, shape((8, LANES), F32), last_gain)
    parts = exchange(parts.reshape(ys, LANES // ys, 2 * hidden + LANES), ("y",), REDUCE)
    act = call(lambda *refs: act_kernel(width, *refs), shape((ys, LANES // ys, hidden), BF), parts)
    act = exchange(act, ("y",), GATHER).reshape(LANES, hidden)
    answers = call(down_kernel, shape((GROUP, 64, LANES), BF), act, scale, *down)
    answers = exchange(answers, ("c", "x"))
    mixed = call(combine_kernel, shape((LANES, local), BF), answers, sel)
    returned = exchange(mixed.reshape(chips, GROUP, local), ("z",))
    combined, squares = call(
        place_kernel,
        [shape((HALF, local), F32), shape((ys * xs, 1, LANES), F32)],
        returned.reshape(LANES, local),
        place,
    )
    squares = exchange(squares, ("y", "x"))
    return call(
        lambda *refs: norm_kernel(width, *refs),
        shape((HALF, local), BF),
        squares,
        combined,
        last_gain,
    )


def solution(mesh):
    fine = Mesh(
        mesh.devices.reshape(mesh.shape["ep"] // 2, 2, mesh.shape["tp"] // 4, 4),
        ("z", "c", "y", "x"),
    )
    ep, tp = ("z", "c"), ("y", "x")
    placed = (
        P(ep, tp),
        P(tp),
        P(tp),
        P(),
        P(),
        P(ep, tp, None),
        P(ep, tp, None),
        P(ep, None, tp),
    )

    return jax.shard_map(on_device, mesh=fine, in_specs=placed, out_specs=P(ep, tp), check_vma=False)
```

```python
import jax
import jax.numpy as jnp
from jax import lax
from jax.experimental import pallas as pl
from jax.experimental.pallas import tpu as pltpu
from jax.sharding import Mesh, PartitionSpec as P

EPS = 1e-06
BF, F32 = jnp.bfloat16, jnp.float32
LANES = 128
HALF = 64
CAP = 4
GROUP = 8
PARAMS = pltpu.CompilerParams(vmem_limit_bytes=16 * 1024 * 1024)
FIRST = {"z": lambda n: 13, "c": lambda n: n - 1, "y": lambda n: n // 2, "x": lambda n: n // 2}
STEP = {"z": 1, "c": 1, "y": 1, "x": 1}
REDUCE = [4, 7, 2, 5, 0, 3, 6, 1]
GATHER = [4, 7, 2, 5, 0, 3, 6, 1]
VMEM = pl.BlockSpec(memory_space=pltpu.VMEM)
HBM = pl.BlockSpec(memory_space=pltpu.HBM)


def in_hbm(value):
    return pltpu.with_memory_space_constraint(value, pltpu.HBM)


def shape(dims, dtype):
    return jax.ShapeDtypeStruct(dims, dtype)


def iota(dims, dim):
    return lax.broadcasted_iota(jnp.int32, dims, dim)


def ones_where(mask, dtype=BF):
    return jnp.where(mask, 1.0, 0.0).astype(dtype)


def earlier():
    s, t = iota((LANES, LANES), 0), iota((LANES, LANES), 1)
    return ones_where((s < t) & ((s >> 6) == (t >> 6)))


def dot(a, b):
    return jnp.dot(a, b, preferred_element_type=F32)


def dot_rows(a, b):
    return lax.dot_general(a, b, (((0,), (0,)), ((), ())), preferred_element_type=F32)


def call(kernel, outs, *args):
    single = not isinstance(outs, (list, tuple))
    return pl.pallas_call(
        kernel,
        out_shape=outs,
        in_specs=[VMEM] * len(args),
        out_specs=VMEM if single else [VMEM] * len(outs),
        compiler_params=PARAMS,
    )(*args)


def place_of(index, axis):
    n = lax.axis_size(axis)
    return lax.rem(index + n - FIRST[axis](n), n)


def named(ids, expert):
    hit = ids[0] == expert
    for k in range(1, CAP):
        hit = hit | (ids[k] == expert)
    return jnp.where(hit, 1.0, 0.0)


def slice_copies(sources, outs, shifts, sems):
    x = lax.axis_index("x")
    return [
        pltpu.make_async_copy(
            source.at[lax.rem(x + d, source.shape[0])],
            out.at[i],
            sems.at[j * len(sources) + i],
        )
        for j, (d, out) in enumerate(zip(shifts, outs))
        for i, source in enumerate(sources)
    ]


def deal(arrays, shifts, kernel=None, extra=(), extra_outs=()):
    one = shape((len(arrays), *arrays[0].shape[1:]), BF)
    n, m, k = len(arrays), len(shifts), len(extra)

    def body(*refs):
        sources, small, rest = refs[:n], refs[n : n + k], refs[n + k :]
        outs, held, sems, small_sems = rest[: len(rest) - k - 2], rest[-k - 2 : -2], *rest[-2:]
        fetches = [
            pltpu.make_async_copy(small[i], held[i], small_sems.at[i]) for i in range(k)
        ]
        copies = slice_copies(sources, outs[:m], shifts, sems)
        for copy in fetches + copies:
            copy.start()
        for copy in fetches:
            copy.wait()
        if kernel is not None:
            kernel(*held, *outs[m:])
        for copy in copies:
            copy.wait()

    return pl.pallas_call(
        body,
        out_shape=[one] * m + list(extra_outs),
        in_specs=[HBM] * (n + k),
        out_specs=[VMEM] * (m + len(extra_outs)),
        scratch_shapes=[pltpu.VMEM(a.shape, a.dtype) for a in extra]
        + [pltpu.SemaphoreType.DMA((m * n,)), pltpu.SemaphoreType.DMA((max(k, 1),))],
        compiler_params=PARAMS,
    )(*[in_hbm(a) for a in (*arrays, *extra)])


def dispatch(ids, tok_ref, out_ref, place_ref):
    z, c = lax.axis_index("z"), lax.axis_index("c")
    chips = ids[0].shape[0]
    first = jnp.sum(jnp.where(iota(ids[0].shape, 0) == z, ids[0], 0), axis=0, keepdims=True)
    group = first >> 3
    member = iota((chips, LANES), 0) == group
    rank = dot(ones_where(member), earlier())
    rank = jnp.sum(jnp.where(member, rank, 0.0), axis=0, keepdims=True).astype(jnp.int32)
    mine = (iota((1, LANES), 1) >> 6) == c
    row = jnp.where(mine, place_of(group, "z") * GROUP + rank, -1)
    place = ones_where(iota((LANES, LANES), 0) == row)
    place_ref[...] = place
    tok = tok_ref[...]
    out_ref[...] = dot(place, jnp.concatenate([tok, tok], axis=0)).astype(BF)


def select_table(ids, sel_ref):
    z, c = lax.axis_index("z"), lax.axis_index("c")
    chips = ids[0].shape[0]
    before = earlier()
    rows = [named(ids, z * GROUP + e) for e in listed(("c", "x"))]
    hits = jnp.concatenate(rows, axis=0)
    anyone = rows[0]
    for e in range(1, GROUP):
        anyone = jnp.maximum(anyone, rows[e])
    rank = dot(hits.astype(BF), before)
    start = (place_of(iota((chips, LANES), 0), "z") * GROUP).astype(F32)
    spot = dot(anyone.astype(BF), before) + start
    spots = jnp.concatenate([spot] * GROUP, axis=0)
    lane = iota((LANES, LANES), 1).astype(F32)
    live = (hits > 0.0) & ((iota((LANES, LANES), 1) >> 6) == c)
    for q in range(CAP):
        at = jnp.sum(jnp.where(live & (rank == q), spots + 1.0, 0.0), axis=1, keepdims=True) - 1.0
        sel_ref[q] = ones_where(lane == at)


def scale_kernel(routes_ref, weights_ref, gain_ref, scale_ref, last_ref):
    z, c, x = lax.axis_index("z"), lax.axis_index("c"), lax.axis_index("x")
    chips = routes_ref.shape[0]
    ids = [routes_ref[:, k, :] for k in range(CAP)]
    own = z * GROUP + c * CAP + x
    hit = named(ids, own)
    rank = dot(hit.astype(BF), earlier())
    weight = jnp.zeros((chips, LANES), F32)
    for k in range(CAP):
        weight = weight + jnp.where(ids[k] == own, weights_ref[:, k, :], 0.0)
    block = iota((chips, LANES), 1) >> 6
    for i, core in enumerate(listed(("c",))):
        for q in range(CAP):
            at = (hit > 0.0) & (rank == q) & (block == core)
            value = jnp.sum(jnp.where(at, weight, 0.0), axis=1, keepdims=True)
            start = (i * CAP + q) * chips
            scale_ref[start : start + chips, :] = jnp.broadcast_to(value, (chips, LANES))
    last_ref[...] = jnp.broadcast_to(gain_ref[...], last_ref.shape)


def three_rows(gain, tail_ref):
    high = gain.astype(BF).astype(F32)
    middle = (gain - high).astype(BF).astype(F32)
    low = gain - high - middle
    row = iota((8, LANES), 0)
    tail = jnp.where(row == 0, high, jnp.where(row == 1, middle, jnp.where(row == 2, low, 0.0)))
    tail_ref[...] = tail.astype(BF)


def routing_kernel(routes_ref, tok_ref, gain_ref, out_ref, place_ref, sel_ref, tail_ref):
    ids = [routes_ref[:, k, :] for k in range(CAP)]
    dispatch(ids, tok_ref, out_ref, place_ref)
    select_table(ids, sel_ref)
    three_rows(gain_ref[...], tail_ref)


def passed(piece, d, axis):
    n = lax.axis_size(axis)
    return lax.ppermute(piece, axis, [(i, (i + d) % n) for i in range(n)])


def select_kernel(recv_ref, sel_ref, tail_ref, out_ref):
    recv = recv_ref[...]
    for q in range(CAP):
        picked = dot(sel_ref[q], recv).astype(BF)
        for e in range(GROUP):
            out_ref[e, q * 16 : (q + 1) * 16, :] = picked[e * 16 : (e + 1) * 16]
    tail = tail_ref[...]
    for e in range(GROUP):
        out_ref[e, 64:72, :] = tail


def gate_up_kernel(rows_ref, *refs):
    *weights, out_ref = refs
    n = len(weights)
    x = lax.axis_index("x")
    squares = jnp.zeros((LANES, 1), F32)
    hidden = weights[0].shape[2]
    gate = jnp.zeros((LANES, hidden), F32)
    up = jnp.zeros((LANES, hidden), F32)
    for d in range(n):
        at = place_of(x - d + n, "x")
        raw = jnp.concatenate([rows_ref[at, 0:64, :], rows_ref[n + at, 0:64, :]], axis=0)
        raw = raw.astype(F32)
        tail = rows_ref[at, 64:72, :].astype(F32)
        gain = tail[0:1] + tail[1:2] + tail[2:3]
        squares = squares + jnp.sum(raw * raw, axis=1, keepdims=True)
        lhs = (raw * gain).astype(BF)
        gate = gate + dot(lhs, weights[d][0])
        up = up + dot(lhs, weights[d][1])
    out_ref[:, 0:hidden] = gate.astype(BF)
    out_ref[:, hidden : 2 * hidden] = up.astype(BF)
    high = squares.astype(BF).astype(F32)
    lane = iota((LANES, LANES), 1)
    out_ref[:, 2 * hidden :] = jnp.where(lane < HALF, high, squares - high).astype(BF)


def act_kernel(width, parts_ref, out_ref):
    total = parts_ref[0].astype(F32)
    for y in range(1, parts_ref.shape[0]):
        total = total + parts_ref[y].astype(F32)
    hidden = out_ref.shape[2]
    squares = total[:, 2 * hidden : 2 * hidden + 1] + total[:, 2 * hidden + HALF : 2 * hidden + HALF + 1]
    scale = lax.rsqrt(squares / width + EPS)
    gate = total[:, 0:hidden] * scale
    up = total[:, hidden : 2 * hidden] * scale
    act = (gate / (1.0 + jnp.exp(-gate)) * up).astype(BF)
    for y in range(out_ref.shape[0]):
        out_ref[y] = act


def slot_rows(act_ref):
    rows = act_ref.shape[0] // len(GATHER)
    at = [GATHER.index(y) * rows for y in REDUCE]
    return jnp.concatenate([act_ref[i : i + rows, :] for i in at], axis=0)


def own_down_kernel(act_ref, scale_ref, weight_ref, out_ref):
    out_ref[...] = (dot(slot_rows(act_ref), weight_ref[0]) * scale_ref[...]).astype(BF)


def down_kernel(act_ref, scale_ref, own_ref, *refs):
    *weights, out_ref = refs
    n = len(weights) + 1
    x = lax.axis_index("x")
    act = slot_rows(act_ref)
    scale = scale_ref[...]
    for d in range(n):
        at = place_of(x - d + n, "x")
        out = (dot(act, weights[d - 1][0]) * scale).astype(BF) if d else own_ref[...]
        out_ref[at] = out[0:64]
        out_ref[n + at] = out[64:128]


def combine_kernel(parts_ref, sel_ref, out_ref):
    total = jnp.zeros((LANES, LANES), F32)
    for q in range(CAP):
        rows = jnp.concatenate(
            [parts_ref[e, q * 16 : (q + 1) * 16, :] for e in range(GROUP)], axis=0
        )
        total = total + dot_rows(sel_ref[q], rows)
    out_ref[...] = total.astype(BF)


def place_kernel(ret_ref, place_ref, comb_ref, squares_ref):
    full = dot_rows(place_ref[...], ret_ref[...])
    comb_ref[...] = full[0:HALF] + full[HALF:LANES]
    squares = jnp.sum(full * full, axis=1, keepdims=True)
    flat = jnp.transpose(jnp.broadcast_to(squares, (LANES, LANES)))[0:1, :]
    for i in range(squares_ref.shape[0]):
        squares_ref[i] = flat


def norm_kernel(width, squares_ref, comb_ref, gain_ref, out_ref):
    total = squares_ref[0]
    for i in range(1, squares_ref.shape[0]):
        total = total + squares_ref[i]
    column = jnp.transpose(jnp.broadcast_to(total, (LANES, LANES)))
    column = column[0:HALF] + column[HALF:LANES]
    out_ref[...] = (comb_ref[...] * lax.rsqrt(column / width + EPS) * gain_ref[0:1, :]).astype(BF)


def listed(axes):
    order = [0]
    for axis in axes:
        n = lax.axis_size(axis)
        order = [i * n + (FIRST[axis](n) + STEP[axis] * k) % n for i in order for k in range(n)]
    return order


def exchange(value, axes, order=None):
    groups = [listed(axes) if order is None else order]
    return lax.all_to_all(value, axes, 0, 0, tiled=True, axis_index_groups=groups)


def on_device(tokens, in_gain, out_gain, routes, route_weights, w_gate, w_up, w_down):
    chips, ys, xs = lax.axis_size("z"), lax.axis_size("y"), lax.axis_size("x")
    local = tokens.shape[1]
    width = float(local * ys * xs)
    hidden = w_gate.shape[2]
    routes = jnp.transpose(routes.reshape(chips, LANES, CAP), (0, 2, 1))
    weights = jnp.transpose(route_weights.reshape(chips, LANES, CAP), (0, 2, 1))

    square = shape((LANES, LANES), BF)
    own, near, far, back, outgoing, place, sel, tail = deal(
        [w_gate, w_up],
        [0, 1, 2, 3],
        routing_kernel,
        (routes, tokens, in_gain.reshape(1, local)),
        (
            square,
            square,
            shape((CAP, LANES, LANES), BF),
            shape((8, LANES), BF),
        ),
    )
    gate_up = [own, passed(near, 1, "x"), passed(far, 2, "x"), passed(back, 3, "x")]
    own, near, far, back = deal([w_down], [0, 1, 2, 3])
    down = [own, passed(near, 1, "x"), passed(far, 2, "x"), passed(back, 3, "x")]
    arrived = exchange(outgoing.reshape(chips, GROUP, local), ("z",))
    slots = call(
        select_kernel, shape((GROUP, 72, LANES), BF), arrived.reshape(LANES, local), sel, tail
    )
    slots = exchange(slots, ("c", "x"))
    parts = call(gate_up_kernel, shape((LANES, 2 * hidden + LANES), BF), slots, *gate_up)
    scale, last_gain = call(
        scale_kernel,
        [shape((LANES, LANES), F32), shape((8, LANES), F32)],
        routes,
        weights,
        out_gain.reshape(1, local),
    )
    parts = exchange(parts.reshape(ys, LANES // ys, 2 * hidden + LANES), ("y",), REDUCE)
    act = call(lambda *refs: act_kernel(width, *refs), shape((ys, LANES // ys, hidden), BF), parts)
    act = exchange(act, ("y",), GATHER).reshape(LANES, hidden)
    own, *others = down
    own = call(own_down_kernel, shape((LANES, LANES), BF), act, scale, own)
    answers = call(down_kernel, shape((GROUP, 64, LANES), BF), act, scale, own, *others)
    answers = exchange(answers, ("c", "x"))
    mixed = call(combine_kernel, shape((LANES, local), BF), answers, sel)
    returned = exchange(mixed.reshape(chips, GROUP, local), ("z",))
    combined, squares = call(
        place_kernel,
        [shape((HALF, local), F32), shape((ys * xs, 1, LANES), F32)],
        returned.reshape(LANES, local),
        place,
    )
    squares = exchange(squares, ("y", "x"))
    return call(
        lambda *refs: norm_kernel(width, *refs),
        shape((HALF, local), BF),
        squares,
        combined,
        last_gain,
    )


def solution(mesh):
    fine = Mesh(
        mesh.devices.reshape(mesh.shape["ep"] // 2, 2, mesh.shape["tp"] // 4, 4),
        ("z", "c", "y", "x"),
    )
    ep, tp = ("z", "c"), ("y", "x")
    placed = (
        P(ep, tp),
        P(tp),
        P(tp),
        P(),
        P(),
        P(ep, tp, None),
        P(ep, tp, None),
        P(ep, None, tp),
    )

    return jax.shard_map(on_device, mesh=fine, in_specs=placed, out_specs=P(ep, tp), check_vma=False)
```

```python
import jax
import jax.numpy as jnp
from jax import lax
from jax.experimental import pallas as pl
from jax.experimental.pallas import tpu as pltpu
from jax.sharding import Mesh, PartitionSpec as P

EPS = 1e-06
BF, F32 = jnp.bfloat16, jnp.float32
LANES = 128
HALF = 64
CAP = 4
GROUP = 8
PARAMS = pltpu.CompilerParams(vmem_limit_bytes=16 * 1024 * 1024)
FIRST = {"z": lambda n: 13, "c": lambda n: n - 1, "y": lambda n: n // 2, "x": lambda n: n // 2}
STEP = {"z": 1, "c": 1, "y": 1, "x": 1}
REDUCE = [4, 7, 2, 5, 0, 3, 6, 1]
GATHER = [4, 7, 2, 5, 0, 3, 6, 1]
VMEM = pl.BlockSpec(memory_space=pltpu.VMEM)
HBM = pl.BlockSpec(memory_space=pltpu.HBM)


def in_hbm(value):
    return pltpu.with_memory_space_constraint(value, pltpu.HBM)


def shape(dims, dtype):
    return jax.ShapeDtypeStruct(dims, dtype)


def iota(dims, dim):
    return lax.broadcasted_iota(jnp.int32, dims, dim)


def ones_where(mask, dtype=BF):
    return jnp.where(mask, 1.0, 0.0).astype(dtype)


def earlier():
    s, t = iota((LANES, LANES), 0), iota((LANES, LANES), 1)
    return ones_where((s < t) & ((s >> 6) == (t >> 6)))


def dot(a, b):
    return jnp.dot(a, b, preferred_element_type=F32)


def dot_rows(a, b):
    return lax.dot_general(a, b, (((0,), (0,)), ((), ())), preferred_element_type=F32)


def call(kernel, outs, *args):
    single = not isinstance(outs, (list, tuple))
    return pl.pallas_call(
        kernel,
        out_shape=outs,
        in_specs=[VMEM] * len(args),
        out_specs=VMEM if single else [VMEM] * len(outs),
        compiler_params=PARAMS,
    )(*args)


def place_of(index, axis):
    n = lax.axis_size(axis)
    return lax.rem(index + n - FIRST[axis](n), n)


def named(ids, expert):
    hit = ids[0] == expert
    for k in range(1, CAP):
        hit = hit | (ids[k] == expert)
    return jnp.where(hit, 1.0, 0.0)


def slice_copies(sources, outs, shifts, sems):
    x = lax.axis_index("x")
    return [
        pltpu.make_async_copy(
            source.at[lax.rem(x + d, source.shape[0])],
            out.at[i],
            sems.at[j * len(sources) + i],
        )
        for j, (d, out) in enumerate(zip(shifts, outs))
        for i, source in enumerate(sources)
    ]


def deal(arrays, shifts, kernel=None, extra=(), extra_outs=()):
    one = shape((len(arrays), *arrays[0].shape[1:]), BF)
    n, m, k = len(arrays), len(shifts), len(extra)

    def body(*refs):
        sources, small, rest = refs[:n], refs[n : n + k], refs[n + k :]
        outs, held, sems, small_sems = rest[: len(rest) - k - 2], rest[-k - 2 : -2], *rest[-2:]
        fetches = [
            pltpu.make_async_copy(small[i], held[i], small_sems.at[i]) for i in range(k)
        ]
        copies = slice_copies(sources, outs[:m], shifts, sems)
        for copy in fetches + copies:
            copy.start()
        for copy in fetches:
            copy.wait()
        if kernel is not None:
            kernel(*held, *outs[m:])
        for copy in copies:
            copy.wait()

    return pl.pallas_call(
        body,
        out_shape=[one] * m + list(extra_outs),
        in_specs=[HBM] * (n + k),
        out_specs=[VMEM] * (m + len(extra_outs)),
        scratch_shapes=[pltpu.VMEM(a.shape, a.dtype) for a in extra]
        + [pltpu.SemaphoreType.DMA((m * n,)), pltpu.SemaphoreType.DMA((max(k, 1),))],
        compiler_params=PARAMS,
    )(*[in_hbm(a) for a in (*arrays, *extra)])


def dispatch(ids, tok_ref, out_ref, place_ref):
    z, c = lax.axis_index("z"), lax.axis_index("c")
    chips = ids[0].shape[0]
    first = jnp.sum(jnp.where(iota(ids[0].shape, 0) == z, ids[0], 0), axis=0, keepdims=True)
    group = first >> 3
    member = iota((chips, LANES), 0) == group
    rank = dot(ones_where(member), earlier())
    rank = jnp.sum(jnp.where(member, rank, 0.0), axis=0, keepdims=True).astype(jnp.int32)
    mine = (iota((1, LANES), 1) >> 6) == c
    row = jnp.where(mine, place_of(group, "z") * GROUP + rank, -1)
    place = ones_where(iota((LANES, LANES), 0) == row)
    place_ref[...] = place
    tok = tok_ref[...]
    out_ref[...] = dot(place, jnp.concatenate([tok, tok], axis=0)).astype(BF)


def select_table(ids, sel_ref):
    z, c = lax.axis_index("z"), lax.axis_index("c")
    chips = ids[0].shape[0]
    before = earlier()
    rows = [named(ids, z * GROUP + e) for e in listed(("c", "x"))]
    hits = jnp.concatenate(rows, axis=0)
    anyone = rows[0]
    for e in range(1, GROUP):
        anyone = jnp.maximum(anyone, rows[e])
    rank = dot(hits.astype(BF), before)
    start = (place_of(iota((chips, LANES), 0), "z") * GROUP).astype(F32)
    spot = dot(anyone.astype(BF), before) + start
    spots = jnp.concatenate([spot] * GROUP, axis=0)
    lane = iota((LANES, LANES), 1).astype(F32)
    live = (hits > 0.0) & ((iota((LANES, LANES), 1) >> 6) == c)
    for q in range(CAP):
        at = jnp.sum(jnp.where(live & (rank == q), spots + 1.0, 0.0), axis=1, keepdims=True) - 1.0
        sel_ref[q] = ones_where(lane == at)


def scale_kernel(routes_ref, weights_ref, gain_ref, scale_ref, last_ref):
    z, c, x = lax.axis_index("z"), lax.axis_index("c"), lax.axis_index("x")
    chips = routes_ref.shape[0]
    ids = [routes_ref[:, k, :] for k in range(CAP)]
    own = z * GROUP + c * CAP + x
    hit = named(ids, own)
    rank = dot(hit.astype(BF), earlier())
    weight = jnp.zeros((chips, LANES), F32)
    for k in range(CAP):
        weight = weight + jnp.where(ids[k] == own, weights_ref[:, k, :], 0.0)
    block = iota((chips, LANES), 1) >> 6
    for i, core in enumerate(listed(("c",))):
        for q in range(CAP):
            at = (hit > 0.0) & (rank == q) & (block == core)
            value = jnp.sum(jnp.where(at, weight, 0.0), axis=1, keepdims=True)
            start = (i * CAP + q) * chips
            scale_ref[start : start + chips, :] = jnp.broadcast_to(value, (chips, LANES))
    last_ref[...] = jnp.broadcast_to(gain_ref[...], last_ref.shape)


def three_rows(gain, tail_ref):
    high = gain.astype(BF).astype(F32)
    middle = (gain - high).astype(BF).astype(F32)
    low = gain - high - middle
    row = iota((8, LANES), 0)
    tail = jnp.where(row == 0, high, jnp.where(row == 1, middle, jnp.where(row == 2, low, 0.0)))
    tail_ref[...] = tail.astype(BF)


def routing_kernel(routes_ref, tok_ref, gain_ref, out_ref, place_ref, sel_ref, tail_ref):
    ids = [routes_ref[:, k, :] for k in range(CAP)]
    dispatch(ids, tok_ref, out_ref, place_ref)
    select_table(ids, sel_ref)
    three_rows(gain_ref[...], tail_ref)


def passed(piece, d, axis):
    n = lax.axis_size(axis)
    return lax.ppermute(piece, axis, [(i, (i + d) % n) for i in range(n)])


def select_kernel(recv_ref, sel_ref, tail_ref, out_ref):
    recv = recv_ref[...]
    for q in range(CAP):
        picked = dot(sel_ref[q], recv).astype(BF)
        for e in range(GROUP):
            out_ref[e, q * 16 : (q + 1) * 16, :] = picked[e * 16 : (e + 1) * 16]
    tail = tail_ref[...]
    for e in range(GROUP):
        out_ref[e, 64:72, :] = tail


def gate_up_kernel(rows_ref, *refs):
    *weights, out_ref = refs
    n = len(weights)
    x = lax.axis_index("x")
    squares = jnp.zeros((LANES, 1), F32)
    hidden = weights[0].shape[2]
    gate = jnp.zeros((LANES, hidden), F32)
    up = jnp.zeros((LANES, hidden), F32)
    for d in range(n):
        at = place_of(x - d + n, "x")
        raw = jnp.concatenate([rows_ref[at, 0:64, :], rows_ref[n + at, 0:64, :]], axis=0)
        raw = raw.astype(F32)
        tail = rows_ref[at, 64:72, :].astype(F32)
        gain = tail[0:1] + tail[1:2] + tail[2:3]
        squares = squares + jnp.sum(raw * raw, axis=1, keepdims=True)
        lhs = (raw * gain).astype(BF)
        gate = gate + dot(lhs, weights[d][0])
        up = up + dot(lhs, weights[d][1])
    ys = out_ref.shape[0]
    share, blocks = LANES // ys, hidden // LANES
    for i, total in enumerate((gate, up)):
        total = total.astype(BF)
        for j in range(blocks):
            part = total[:, j * LANES : (j + 1) * LANES]
            at = (i * blocks + j) * share
            for y in range(ys):
                out_ref[y, at : at + share, :] = part[y * share : (y + 1) * share]
    high = squares.astype(BF).astype(F32)
    low = squares - high
    lane = iota((8, LANES), 1)
    for y in range(ys):
        start = y * share
        first, second = slice(start, start + 8), slice(start + 8, start + 16)
        out_ref[y, 2 * blocks * share :, :] = jnp.where(
            lane < 32,
            high[first],
            jnp.where(lane < 64, low[first], jnp.where(lane < 96, high[second], low[second])),
        ).astype(BF)


def act_kernel(width, parts_ref, out_ref):
    ys, rows, _ = parts_ref.shape
    total = parts_ref[0].astype(F32)
    for y in range(1, ys):
        total = total + parts_ref[y].astype(F32)
    share = out_ref.shape[1] // ((rows - 8) // (2 * 16))
    tail = total[rows - 8 :]
    squares = jnp.concatenate(
        [tail[:, 0:1] + tail[:, 32:33], tail[:, 64:65] + tail[:, 96:97]], axis=0
    )
    scale = lax.rsqrt(squares / width + EPS)
    half = (rows - 8) // 2
    for j in range(half // share):
        gate = total[j * share : (j + 1) * share] * scale
        up = total[half + j * share : half + (j + 1) * share] * scale
        act = (gate / (1.0 + jnp.exp(-gate)) * up).astype(BF)
        for y in range(ys):
            out_ref[y, j * share : (j + 1) * share, :] = act


def slot_rows(act_ref):
    ys, rows, _ = act_ref.shape
    share = LANES // ys
    at = [GATHER.index(y) for y in REDUCE]
    return jnp.concatenate(
        [
            jnp.concatenate([act_ref[i, j : j + share, :] for i in at], axis=0)
            for j in range(0, rows, share)
        ],
        axis=1,
    )


def own_down_kernel(act_ref, scale_ref, weight_ref, out_ref):
    out_ref[...] = (dot(slot_rows(act_ref), weight_ref[0]) * scale_ref[...]).astype(BF)


def down_kernel(act_ref, scale_ref, own_ref, *refs):
    *weights, out_ref = refs
    n = len(weights) + 1
    x = lax.axis_index("x")
    act = slot_rows(act_ref)
    scale = scale_ref[...]
    for d in range(n):
        at = place_of(x - d + n, "x")
        out = (dot(act, weights[d - 1][0]) * scale).astype(BF) if d else own_ref[...]
        out_ref[at] = out[0:64]
        out_ref[n + at] = out[64:128]


def combine_kernel(parts_ref, sel_ref, out_ref):
    total = jnp.zeros((LANES, LANES), F32)
    for q in range(CAP):
        rows = jnp.concatenate(
            [parts_ref[e, q * 16 : (q + 1) * 16, :] for e in range(GROUP)], axis=0
        )
        total = total + dot_rows(sel_ref[q], rows)
    out_ref[...] = total.astype(BF)


def place_kernel(ret_ref, place_ref, comb_ref, squares_ref):
    full = dot_rows(place_ref[...], ret_ref[...])
    comb_ref[...] = full[0:HALF] + full[HALF:LANES]
    squares = jnp.sum(full * full, axis=1, keepdims=True)
    flat = jnp.transpose(jnp.broadcast_to(squares, (LANES, LANES)))[0:1, :]
    for i in range(squares_ref.shape[0]):
        squares_ref[i] = flat


def norm_kernel(width, squares_ref, comb_ref, gain_ref, out_ref):
    total = squares_ref[0]
    for i in range(1, squares_ref.shape[0]):
        total = total + squares_ref[i]
    column = jnp.transpose(jnp.broadcast_to(total, (LANES, LANES)))
    column = column[0:HALF] + column[HALF:LANES]
    out_ref[...] = (comb_ref[...] * lax.rsqrt(column / width + EPS) * gain_ref[0:1, :]).astype(BF)


def listed(axes):
    order = [0]
    for axis in axes:
        n = lax.axis_size(axis)
        order = [i * n + (FIRST[axis](n) + STEP[axis] * k) % n for i in order for k in range(n)]
    return order


def exchange(value, axes, order=None):
    groups = [listed(axes) if order is None else order]
    return lax.all_to_all(value, axes, 0, 0, tiled=True, axis_index_groups=groups)


def on_device(tokens, in_gain, out_gain, routes, route_weights, w_gate, w_up, w_down):
    chips, ys, xs = lax.axis_size("z"), lax.axis_size("y"), lax.axis_size("x")
    local = tokens.shape[1]
    width = float(local * ys * xs)
    hidden = w_gate.shape[2]
    routes = jnp.transpose(routes.reshape(chips, LANES, CAP), (0, 2, 1))
    weights = jnp.transpose(route_weights.reshape(chips, LANES, CAP), (0, 2, 1))

    square = shape((LANES, LANES), BF)
    own, near, far, back, outgoing, place, sel, tail = deal(
        [w_gate, w_up],
        [0, 1, 2, 3],
        routing_kernel,
        (routes, tokens, in_gain.reshape(1, local)),
        (
            square,
            square,
            shape((CAP, LANES, LANES), BF),
            shape((8, LANES), BF),
        ),
    )
    gate_up = [own, passed(near, 1, "x"), passed(far, 2, "x"), passed(back, 3, "x")]
    own, near, far, back = deal([w_down], [0, 1, 2, 3])
    down = [own, passed(near, 1, "x"), passed(far, 2, "x"), passed(back, 3, "x")]
    arrived = exchange(outgoing.reshape(chips, GROUP, local), ("z",))
    slots = call(
        select_kernel, shape((GROUP, 72, LANES), BF), arrived.reshape(LANES, local), sel, tail
    )
    slots = exchange(slots, ("c", "x"))
    share = LANES // ys
    parts = call(
        gate_up_kernel, shape((ys, 2 * hidden // LANES * share + 8, LANES), BF), slots, *gate_up
    )
    scale, last_gain = call(
        scale_kernel,
        [shape((LANES, LANES), F32), shape((8, LANES), F32)],
        routes,
        weights,
        out_gain.reshape(1, local),
    )
    parts = exchange(parts, ("y",), REDUCE)
    act = call(
        lambda *refs: act_kernel(width, *refs),
        shape((ys, hidden // LANES * share, LANES), BF),
        parts,
    )
    act = exchange(act, ("y",), GATHER)
    own, *others = down
    own = call(own_down_kernel, shape((LANES, LANES), BF), act, scale, own)
    answers = call(down_kernel, shape((GROUP, 64, LANES), BF), act, scale, own, *others)
    answers = exchange(answers, ("c", "x"))
    mixed = call(combine_kernel, shape((LANES, local), BF), answers, sel)
    returned = exchange(mixed.reshape(chips, GROUP, local), ("z",))
    combined, squares = call(
        place_kernel,
        [shape((HALF, local), F32), shape((ys * xs, 1, LANES), F32)],
        returned.reshape(LANES, local),
        place,
    )
    squares = exchange(squares, ("y", "x"))
    return call(
        lambda *refs: norm_kernel(width, *refs),
        shape((HALF, local), BF),
        squares,
        combined,
        last_gain,
    )


def solution(mesh):
    fine = Mesh(
        mesh.devices.reshape(mesh.shape["ep"] // 2, 2, mesh.shape["tp"] // 4, 4),
        ("z", "c", "y", "x"),
    )
    ep, tp = ("z", "c"), ("y", "x")
    placed = (
        P(ep, tp),
        P(tp),
        P(tp),
        P(),
        P(),
        P(ep, tp, None),
        P(ep, tp, None),
        P(ep, None, tp),
    )

    return jax.shard_map(on_device, mesh=fine, in_specs=placed, out_specs=P(ep, tp), check_vma=False)
```

```python
import jax
import jax.numpy as jnp
from jax import lax
from jax.experimental import pallas as pl
from jax.experimental.pallas import tpu as pltpu
from jax.sharding import Mesh, PartitionSpec as P

EPS = 1e-06
BF, F32 = jnp.bfloat16, jnp.float32
LANES = 128
HALF = 64
CAP = 4
GROUP = 8
PARAMS = pltpu.CompilerParams(vmem_limit_bytes=16 * 1024 * 1024)
FIRST = {"z": lambda n: 15, "c": lambda n: n - 1, "y": lambda n: n // 2, "x": lambda n: n // 2}
STEP = {"z": 1, "c": 1, "y": 1, "x": 1}
BACK = 8
REDUCE = [4, 7, 2, 5, 0, 3, 6, 1]
GATHER = [4, 7, 2, 5, 0, 3, 6, 1]
VMEM = pl.BlockSpec(memory_space=pltpu.VMEM)
HBM = pl.BlockSpec(memory_space=pltpu.HBM)


def in_hbm(value):
    return pltpu.with_memory_space_constraint(value, pltpu.HBM)


def shape(dims, dtype):
    return jax.ShapeDtypeStruct(dims, dtype)


def iota(dims, dim):
    return lax.broadcasted_iota(jnp.int32, dims, dim)


def ones_where(mask, dtype=BF):
    return jnp.where(mask, 1.0, 0.0).astype(dtype)


def earlier():
    s, t = iota((LANES, LANES), 0), iota((LANES, LANES), 1)
    return ones_where((s < t) & ((s >> 6) == (t >> 6)))


def dot(a, b):
    return jnp.dot(a, b, preferred_element_type=F32)


def dot_rows(a, b):
    return lax.dot_general(a, b, (((0,), (0,)), ((), ())), preferred_element_type=F32)


def call(kernel, outs, *args):
    single = not isinstance(outs, (list, tuple))
    return pl.pallas_call(
        kernel,
        out_shape=outs,
        in_specs=[VMEM] * len(args),
        out_specs=VMEM if single else [VMEM] * len(outs),
        compiler_params=PARAMS,
    )(*args)


def turned(rows, chips, first):
    at = (first - FIRST["z"](chips)) % chips * (rows.shape[0] // chips)
    return jnp.concatenate([rows[at:], rows[:at]], axis=0) if at else rows


def place_of(index, axis):
    n = lax.axis_size(axis)
    return lax.rem(index + n - FIRST[axis](n), n)


def named(ids, expert):
    hit = ids[0] == expert
    for k in range(1, CAP):
        hit = hit | (ids[k] == expert)
    return jnp.where(hit, 1.0, 0.0)


def slice_copies(sources, outs, shifts, sems):
    x = lax.axis_index("x")
    return [
        pltpu.make_async_copy(
            source.at[lax.rem(x + d, source.shape[0])],
            out.at[i],
            sems.at[j * len(sources) + i],
        )
        for j, (d, out) in enumerate(zip(shifts, outs))
        for i, source in enumerate(sources)
    ]


def deal(arrays, shifts, kernels=(), extra=(), extra_outs=(), out=()):
    one = shape((len(arrays), *arrays[0].shape[1:]), BF)
    n, m, k = len(arrays), len(shifts), len(extra)
    through = [shifts.index(d) for d in out] + ([m] if out else [])
    shapes = [one] * m + list(extra_outs)

    def body(*refs):
        sources, small, rest = refs[:n], refs[n : n + k], refs[n + k :]
        outs, rest = list(rest[: len(shapes)]), rest[len(shapes) :]
        held, kept, (sems, small_sems, out_sems) = rest[:k], rest[k:-3], rest[-3:]
        stores = []
        for i, at in enumerate(through):
            stores.append(pltpu.make_async_copy(kept[i], outs[at], out_sems.at[i]))
            outs[at] = kept[i]
        fetches = [
            pltpu.make_async_copy(small[i], held[i], small_sems.at[i]) for i in range(k)
        ]
        copies = slice_copies(sources, outs[:m], shifts, sems)
        ahead = sorted(range(m * n), key=lambda i: i // n not in through)
        for copy in fetches + [copies[i] for i in ahead]:
            copy.start()
        for copy in fetches:
            copy.wait()
        for i, step in enumerate(kernels):
            step(*held, *outs[m:])
            if i == 0:
                for store, at in reversed(list(zip(stores, through))):
                    for copy in copies[at * n : (at + 1) * n]:
                        copy.wait()
                    store.start()
        for i, copy in enumerate(copies):
            if i // n not in through:
                copy.wait()
        for store in stores:
            store.wait()

    return pl.pallas_call(
        body,
        out_shape=shapes,
        in_specs=[HBM] * (n + k),
        out_specs=[HBM if i in through else VMEM for i in range(len(shapes))],
        scratch_shapes=[pltpu.VMEM(a.shape, a.dtype) for a in extra]
        + [pltpu.VMEM(shapes[i].shape, BF) for i in through]
        + [
            pltpu.SemaphoreType.DMA((m * n,)),
            pltpu.SemaphoreType.DMA((max(k, 1),)),
            pltpu.SemaphoreType.DMA((max(len(through), 1),)),
        ],
        compiler_params=PARAMS,
    )(*[in_hbm(a) for a in (*arrays, *extra)])


def dispatch(ids, tok_ref, out_ref, place_ref):
    z, c = lax.axis_index("z"), lax.axis_index("c")
    chips = ids[0].shape[0]
    first = jnp.sum(jnp.where(iota(ids[0].shape, 0) == z, ids[0], 0), axis=0, keepdims=True)
    group = first >> 3
    member = iota((chips, LANES), 0) == group
    rank = dot(ones_where(member), earlier())
    rank = jnp.sum(jnp.where(member, rank, 0.0), axis=0, keepdims=True).astype(jnp.int32)
    mine = (iota((1, LANES), 1) >> 6) == c
    row = jnp.where(mine, place_of(group, "z") * GROUP + rank, -1)
    place = ones_where(iota((LANES, LANES), 0) == row)
    place_ref[...] = place
    tok = tok_ref[...]
    out_ref[...] = dot(place, jnp.concatenate([tok, tok], axis=0)).astype(BF)


def select_table(ids, sel_ref):
    z, c = lax.axis_index("z"), lax.axis_index("c")
    chips = ids[0].shape[0]
    before = earlier()
    rows = [named(ids, z * GROUP + e) for e in listed(("c", "x"))]
    hits = jnp.concatenate(rows, axis=0)
    anyone = rows[0]
    for e in range(1, GROUP):
        anyone = jnp.maximum(anyone, rows[e])
    rank = dot(hits.astype(BF), before)
    start = (place_of(iota((chips, LANES), 0), "z") * GROUP).astype(F32)
    spot = dot(anyone.astype(BF), before) + start
    spots = jnp.concatenate([spot] * GROUP, axis=0)
    lane = iota((LANES, LANES), 1).astype(F32)
    live = (hits > 0.0) & ((iota((LANES, LANES), 1) >> 6) == c)
    for q in range(CAP):
        at = jnp.sum(jnp.where(live & (rank == q), spots + 1.0, 0.0), axis=1, keepdims=True) - 1.0
        sel_ref[q] = ones_where(lane == at)


def scale_kernel(routes_ref, weights_ref, gain_ref, scale_ref, last_ref):
    z, c, x = lax.axis_index("z"), lax.axis_index("c"), lax.axis_index("x")
    chips = routes_ref.shape[0]
    ids = [routes_ref[:, k, :] for k in range(CAP)]
    own = z * GROUP + c * CAP + x
    hit = named(ids, own)
    rank = dot(hit.astype(BF), earlier())
    weight = jnp.zeros((chips, LANES), F32)
    for k in range(CAP):
        weight = weight + jnp.where(ids[k] == own, weights_ref[:, k, :], 0.0)
    block = iota((chips, LANES), 1) >> 6
    for i, core in enumerate(listed(("c",))):
        for q in range(CAP):
            at = (hit > 0.0) & (rank == q) & (block == core)
            value = jnp.sum(jnp.where(at, weight, 0.0), axis=1, keepdims=True)
            start = (i * CAP + q) * chips
            scale_ref[start : start + chips, :] = jnp.broadcast_to(value, (chips, LANES))
    last_ref[...] = jnp.broadcast_to(gain_ref[...], last_ref.shape)


def tail_kernel(gain_ref, tail_ref):
    gain = gain_ref[...]
    high = gain.astype(BF).astype(F32)
    middle = (gain - high).astype(BF).astype(F32)
    low = gain - high - middle
    row = iota((8, LANES), 0)
    tail = jnp.where(row == 0, high, jnp.where(row == 1, middle, jnp.where(row == 2, low, 0.0)))
    tail_ref[...] = tail.astype(BF)


def dispatch_step(routes_ref, tok_ref, out_ref, place_ref, sel_ref):
    dispatch([routes_ref[:, k, :] for k in range(CAP)], tok_ref, out_ref, place_ref)


def select_step(routes_ref, tok_ref, out_ref, place_ref, sel_ref):
    select_table([routes_ref[:, k, :] for k in range(CAP)], sel_ref)


def passed(piece, d, axis):
    n = lax.axis_size(axis)
    return lax.ppermute(piece, axis, [(i, (i + d) % n) for i in range(n)])


def select_kernel(recv_ref, sel_ref, tail_ref, out_ref):
    recv = recv_ref[...]
    for q in range(CAP):
        picked = dot(sel_ref[q], recv).astype(BF)
        for e in range(GROUP):
            out_ref[e, q * 16 : (q + 1) * 16, :] = picked[e * 16 : (e + 1) * 16]
    tail = tail_ref[...]
    for e in range(GROUP):
        out_ref[e, 64:72, :] = tail


def gate_up_kernel(rows_ref, *refs):
    *weights, out_ref = refs
    n = len(weights)
    x = lax.axis_index("x")
    squares = jnp.zeros((LANES, 1), F32)
    hidden = weights[0].shape[2]
    gate = jnp.zeros((LANES, hidden), F32)
    up = jnp.zeros((LANES, hidden), F32)
    for d in range(n):
        at = place_of(x - d + n, "x")
        raw = jnp.concatenate([rows_ref[at, 0:64, :], rows_ref[n + at, 0:64, :]], axis=0)
        raw = raw.astype(F32)
        tail = rows_ref[at, 64:72, :].astype(F32)
        gain = tail[0:1] + tail[1:2] + tail[2:3]
        squares = squares + jnp.sum(raw * raw, axis=1, keepdims=True)
        lhs = (raw * gain).astype(BF)
        gate = gate + dot(lhs, weights[d][0])
        up = up + dot(lhs, weights[d][1])
    ys = out_ref.shape[0]
    share, blocks = LANES // ys, hidden // LANES
    for i, total in enumerate((gate, up)):
        total = total.astype(BF)
        for j in range(blocks):
            part = total[:, j * LANES : (j + 1) * LANES]
            at = (i * blocks + j) * share
            for y in range(ys):
                out_ref[y, at : at + share, :] = part[y * share : (y + 1) * share]
    high = squares.astype(BF).astype(F32)
    low = squares - high
    lane = iota((8, LANES), 1)
    for y in range(ys):
        start = y * share
        first, second = slice(start, start + 8), slice(start + 8, start + 16)
        out_ref[y, 2 * blocks * share :, :] = jnp.where(
            lane < 32,
            high[first],
            jnp.where(lane < 64, low[first], jnp.where(lane < 96, high[second], low[second])),
        ).astype(BF)


def act_kernel(width, parts_ref, out_ref):
    ys, rows, _ = parts_ref.shape
    total = parts_ref[0].astype(F32)
    for y in range(1, ys):
        total = total + parts_ref[y].astype(F32)
    share = out_ref.shape[1] // ((rows - 8) // (2 * 16))
    tail = total[rows - 8 :]
    squares = jnp.concatenate(
        [tail[:, 0:1] + tail[:, 32:33], tail[:, 64:65] + tail[:, 96:97]], axis=0
    )
    scale = lax.rsqrt(squares / width + EPS)
    half = (rows - 8) // 2
    for j in range(half // share):
        gate = total[j * share : (j + 1) * share] * scale
        up = total[half + j * share : half + (j + 1) * share] * scale
        act = (gate / (1.0 + jnp.exp(-gate)) * up).astype(BF)
        for y in range(ys):
            out_ref[y, j * share : (j + 1) * share, :] = act


def slot_rows(act_ref):
    ys, rows, _ = act_ref.shape
    share = LANES // ys
    at = [GATHER.index(y) for y in REDUCE]
    return jnp.concatenate(
        [
            jnp.concatenate([act_ref[i, j : j + share, :] for i in at], axis=0)
            for j in range(0, rows, share)
        ],
        axis=1,
    )


def own_down_kernel(act_ref, scale_ref, weight_ref, out_ref):
    out_ref[...] = (dot(slot_rows(act_ref), weight_ref[0]) * scale_ref[...]).astype(BF)


def down_kernel(act_ref, scale_ref, own_ref, *refs):
    *weights, out_ref = refs
    n = len(weights) + 1
    x = lax.axis_index("x")
    act = slot_rows(act_ref)
    scale = scale_ref[...]
    for d in range(n):
        at = place_of(x - d + n, "x")
        out = (dot(act, weights[d - 1][0]) * scale).astype(BF) if d else own_ref[...]
        out_ref[at] = out[0:64]
        out_ref[n + at] = out[64:128]


def combine_kernel(parts_ref, sel_ref, out_ref):
    total = jnp.zeros((LANES, LANES), F32)
    for q in range(CAP):
        rows = jnp.concatenate(
            [parts_ref[e, q * 16 : (q + 1) * 16, :] for e in range(GROUP)], axis=0
        )
        total = total + dot_rows(sel_ref[q], rows)
    out_ref[...] = turned(total, lax.axis_size("z"), BACK).astype(BF)


def place_kernel(ret_ref, place_ref, comb_ref, squares_ref):
    chips = lax.axis_size("z")
    back = turned(ret_ref[...], chips, 2 * FIRST["z"](chips) - BACK)
    full = dot_rows(place_ref[...], back)
    comb_ref[...] = full[0:HALF] + full[HALF:LANES]
    squares = jnp.sum(full * full, axis=1, keepdims=True)
    flat = jnp.transpose(jnp.broadcast_to(squares, (LANES, LANES)))[0:1, :]
    for i in range(squares_ref.shape[0]):
        squares_ref[i] = flat


def norm_kernel(width, squares_ref, comb_ref, gain_ref, out_ref):
    total = squares_ref[0]
    for i in range(1, squares_ref.shape[0]):
        total = total + squares_ref[i]
    column = jnp.transpose(jnp.broadcast_to(total, (LANES, LANES)))
    column = column[0:HALF] + column[HALF:LANES]
    out_ref[...] = (comb_ref[...] * lax.rsqrt(column / width + EPS) * gain_ref[0:1, :]).astype(BF)


def listed(axes):
    order = [0]
    for axis in axes:
        n = lax.axis_size(axis)
        order = [i * n + (FIRST[axis](n) + STEP[axis] * k) % n for i in order for k in range(n)]
    return order


def exchange(value, axes, order=None):
    groups = [listed(axes) if order is None else order]
    return lax.all_to_all(value, axes, 0, 0, tiled=True, axis_index_groups=groups)


def on_device(tokens, in_gain, out_gain, routes, route_weights, w_gate, w_up, w_down):
    chips, ys, xs = lax.axis_size("z"), lax.axis_size("y"), lax.axis_size("x")
    local = tokens.shape[1]
    width = float(local * ys * xs)
    hidden = w_gate.shape[2]
    routes = jnp.transpose(routes.reshape(chips, LANES, CAP), (0, 2, 1))
    weights = jnp.transpose(route_weights.reshape(chips, LANES, CAP), (0, 2, 1))

    square = shape((LANES, LANES), BF)
    own, near, far, back, outgoing, place, sel = deal(
        [w_gate, w_up],
        [0, 1, 2, 3],
        (dispatch_step, select_step),
        (routes, tokens),
        (
            square,
            square,
            shape((CAP, LANES, LANES), BF),
        ),
        out=(1,),
    )
    gate_up = [own, passed(near, 1, "x"), passed(far, 2, "x"), passed(back, 3, "x")]
    own, near, far, back = deal([w_down], [0, 1, 2, 3])
    down = [own, passed(near, 1, "x"), passed(far, 2, "x"), passed(back, 3, "x")]
    tail = call(tail_kernel, shape((8, LANES), BF), in_gain.reshape(1, local))
    arrived = exchange(outgoing.reshape(chips, GROUP, local), ("z",))
    slots = call(
        select_kernel, shape((GROUP, 72, LANES), BF), arrived.reshape(LANES, local), sel, tail
    )
    slots = exchange(slots, ("c", "x"))
    share = LANES // ys
    parts = call(
        gate_up_kernel, shape((ys, 2 * hidden // LANES * share + 8, LANES), BF), slots, *gate_up
    )
    scale, last_gain = call(
        scale_kernel,
        [shape((LANES, LANES), F32), shape((8, LANES), F32)],
        routes,
        weights,
        out_gain.reshape(1, local),
    )
    parts = exchange(parts, ("y",), REDUCE)
    act = call(
        lambda *refs: act_kernel(width, *refs),
        shape((ys, hidden // LANES * share, LANES), BF),
        parts,
    )
    act = exchange(act, ("y",), GATHER)
    own, *others = down
    own = call(own_down_kernel, shape((LANES, LANES), BF), act, scale, own)
    answers = call(down_kernel, shape((GROUP, 64, LANES), BF), act, scale, own, *others)
    answers = exchange(answers, ("c", "x"))
    mixed = call(combine_kernel, shape((LANES, local), BF), answers, sel)
    order = [(BACK + i) % chips for i in range(chips)]
    returned = exchange(mixed.reshape(chips, GROUP, local), ("z",), order)
    combined, squares = call(
        place_kernel,
        [shape((HALF, local), F32), shape((ys * xs, 1, LANES), F32)],
        returned.reshape(LANES, local),
        place,
    )
    squares = exchange(squares, ("y", "x"))
    return call(
        lambda *refs: norm_kernel(width, *refs),
        shape((HALF, local), BF),
        squares,
        combined,
        last_gain,
    )


def solution(mesh):
    fine = Mesh(
        mesh.devices.reshape(mesh.shape["ep"] // 2, 2, mesh.shape["tp"] // 4, 4),
        ("z", "c", "y", "x"),
    )
    ep, tp = ("z", "c"), ("y", "x")
    placed = (
        P(ep, tp),
        P(tp),
        P(tp),
        P(),
        P(),
        P(ep, tp, None),
        P(ep, tp, None),
        P(ep, None, tp),
    )

    return jax.shard_map(on_device, mesh=fine, in_specs=placed, out_specs=P(ep, tp), check_vma=False)
```

```python
import jax
import jax.numpy as jnp
from jax import lax
from jax.experimental import pallas as pl
from jax.experimental.pallas import tpu as pltpu
from jax.sharding import Mesh, PartitionSpec as P

EPS = 1e-06
BF, F32 = jnp.bfloat16, jnp.float32
LANES = 128
HALF = 64
CAP = 4
GROUP = 8
PARAMS = pltpu.CompilerParams(vmem_limit_bytes=16 * 1024 * 1024)
FIRST = {"z": lambda n: 15, "c": lambda n: n - 1, "y": lambda n: n // 2, "x": lambda n: n // 2}
STEP = {"z": 1, "c": 1, "y": 1, "x": 1}
BACK = 8
REDUCE = [4, 7, 2, 5, 0, 3, 6, 1]
GATHER = [4, 7, 2, 5, 0, 3, 6, 1]
VMEM = pl.BlockSpec(memory_space=pltpu.VMEM)
HBM = pl.BlockSpec(memory_space=pltpu.HBM)


def in_hbm(value):
    return pltpu.with_memory_space_constraint(value, pltpu.HBM)


def shape(dims, dtype):
    return jax.ShapeDtypeStruct(dims, dtype)


def iota(dims, dim):
    return lax.broadcasted_iota(jnp.int32, dims, dim)


def ones_where(mask, dtype=BF):
    return jnp.where(mask, 1.0, 0.0).astype(dtype)


def earlier():
    s, t = iota((LANES, LANES), 0), iota((LANES, LANES), 1)
    return ones_where((s < t) & ((s >> 6) == (t >> 6)))


def dot(a, b):
    return jnp.dot(a, b, preferred_element_type=F32)


def dot_rows(a, b):
    return lax.dot_general(a, b, (((0,), (0,)), ((), ())), preferred_element_type=F32)


def call(kernel, outs, *args):
    single = not isinstance(outs, (list, tuple))
    return pl.pallas_call(
        kernel,
        out_shape=outs,
        in_specs=[VMEM] * len(args),
        out_specs=VMEM if single else [VMEM] * len(outs),
        compiler_params=PARAMS,
    )(*args)


def turned(rows, chips, first):
    at = (first - FIRST["z"](chips)) % chips * (rows.shape[0] // chips)
    return jnp.concatenate([rows[at:], rows[:at]], axis=0) if at else rows


def place_of(index, axis):
    n = lax.axis_size(axis)
    return lax.rem(index + n - FIRST[axis](n), n)


def named(ids, expert):
    hit = ids[0] == expert
    for k in range(1, CAP):
        hit = hit | (ids[k] == expert)
    return jnp.where(hit, 1.0, 0.0)


def slice_copies(sources, outs, shifts, sems):
    x = lax.axis_index("x")
    return [
        pltpu.make_async_copy(
            source.at[lax.rem(x + d, source.shape[0])],
            out.at[i],
            sems.at[j * len(sources) + i],
        )
        for j, (d, out) in enumerate(zip(shifts, outs))
        for i, source in enumerate(sources)
    ]


def deal(arrays, shifts, kernels=(), extra=(), extra_outs=(), out=()):
    one = shape((len(arrays), *arrays[0].shape[1:]), BF)
    n, m, k = len(arrays), len(shifts), len(extra)
    through = [shifts.index(d) for d in out] + ([m] if out else [])
    shapes = [one] * m + list(extra_outs)

    def body(*refs):
        sources, small, rest = refs[:n], refs[n : n + k], refs[n + k :]
        outs, rest = list(rest[: len(shapes)]), rest[len(shapes) :]
        held, kept, (sems, small_sems, out_sems) = rest[:k], rest[k:-3], rest[-3:]
        stores = []
        for i, at in enumerate(through):
            stores.append(pltpu.make_async_copy(kept[i], outs[at], out_sems.at[i]))
            outs[at] = kept[i]
        fetches = [
            pltpu.make_async_copy(small[i], held[i], small_sems.at[i]) for i in range(k)
        ]
        copies = slice_copies(sources, outs[:m], shifts, sems)
        ahead = sorted(range(m * n), key=lambda i: i // n not in through)
        for copy in fetches + [copies[i] for i in ahead]:
            copy.start()
        for copy in fetches:
            copy.wait()
        for i, step in enumerate(kernels):
            step(*held, *outs[m:])
            if i == 0:
                for store, at in reversed(list(zip(stores, through))):
                    for copy in copies[at * n : (at + 1) * n]:
                        copy.wait()
                    store.start()
        for i, copy in enumerate(copies):
            if i // n not in through:
                copy.wait()
        for store in stores:
            store.wait()

    return pl.pallas_call(
        body,
        out_shape=shapes,
        in_specs=[HBM] * (n + k),
        out_specs=[HBM if i in through else VMEM for i in range(len(shapes))],
        scratch_shapes=[pltpu.VMEM(a.shape, a.dtype) for a in extra]
        + [pltpu.VMEM(shapes[i].shape, BF) for i in through]
        + [
            pltpu.SemaphoreType.DMA((m * n,)),
            pltpu.SemaphoreType.DMA((max(k, 1),)),
            pltpu.SemaphoreType.DMA((max(len(through), 1),)),
        ],
        compiler_params=PARAMS,
    )(*[in_hbm(a) for a in (*arrays, *extra)])


def dispatch(ids, tok_ref, out_ref, place_ref):
    z, c = lax.axis_index("z"), lax.axis_index("c")
    chips = ids[0].shape[0]
    first = jnp.sum(jnp.where(iota(ids[0].shape, 0) == z, ids[0], 0), axis=0, keepdims=True)
    group = first >> 3
    member = iota((chips, LANES), 0) == group
    rank = dot(ones_where(member), earlier())
    rank = jnp.sum(jnp.where(member, rank, 0.0), axis=0, keepdims=True).astype(jnp.int32)
    mine = (iota((1, LANES), 1) >> 6) == c
    row = jnp.where(mine, place_of(group, "z") * GROUP + rank, -1)
    place = ones_where(iota((LANES, LANES), 0) == row)
    place_ref[...] = place
    tok = tok_ref[...]
    out_ref[...] = dot(place, jnp.concatenate([tok, tok], axis=0)).astype(BF)


def select_table(ids, sel_ref):
    z, c = lax.axis_index("z"), lax.axis_index("c")
    chips = ids[0].shape[0]
    before = earlier()
    rows = [named(ids, z * GROUP + e) for e in listed(("c", "x"))]
    hits = jnp.concatenate(rows, axis=0)
    anyone = rows[0]
    for e in range(1, GROUP):
        anyone = jnp.maximum(anyone, rows[e])
    rank = dot(hits.astype(BF), before)
    start = (place_of(iota((chips, LANES), 0), "z") * GROUP).astype(F32)
    spot = dot(anyone.astype(BF), before) + start
    spots = jnp.concatenate([spot] * GROUP, axis=0)
    lane = iota((LANES, LANES), 1).astype(F32)
    live = (hits > 0.0) & ((iota((LANES, LANES), 1) >> 6) == c)
    for q in range(CAP):
        at = jnp.sum(jnp.where(live & (rank == q), spots + 1.0, 0.0), axis=1, keepdims=True) - 1.0
        sel_ref[q] = ones_where(lane == at)


def scale_kernel(routes_ref, weights_ref, gain_ref, scale_ref, last_ref):
    z, c, x = lax.axis_index("z"), lax.axis_index("c"), lax.axis_index("x")
    chips = routes_ref.shape[0]
    ids = [routes_ref[:, k, :] for k in range(CAP)]
    own = z * GROUP + c * CAP + x
    hit = named(ids, own)
    rank = dot(hit.astype(BF), earlier())
    weight = jnp.zeros((chips, LANES), F32)
    for k in range(CAP):
        weight = weight + jnp.where(ids[k] == own, weights_ref[:, k, :], 0.0)
    block = iota((chips, LANES), 1) >> 6
    for i, core in enumerate(listed(("c",))):
        for q in range(CAP):
            at = (hit > 0.0) & (rank == q) & (block == core)
            value = jnp.sum(jnp.where(at, weight, 0.0), axis=1, keepdims=True)
            start = (i * CAP + q) * chips
            scale_ref[start : start + chips, :] = jnp.broadcast_to(value, (chips, LANES))
    last_ref[...] = jnp.broadcast_to(gain_ref[...], last_ref.shape)


def tail_kernel(gain_ref, tail_ref):
    gain = gain_ref[...]
    high = gain.astype(BF).astype(F32)
    middle = (gain - high).astype(BF).astype(F32)
    low = gain - high - middle
    row = iota((8, LANES), 0)
    tail = jnp.where(row == 0, high, jnp.where(row == 1, middle, jnp.where(row == 2, low, 0.0)))
    tail_ref[...] = tail.astype(BF)


def dispatch_step(routes_ref, tok_ref, out_ref, place_ref):
    dispatch([routes_ref[:, k, :] for k in range(CAP)], tok_ref, out_ref, place_ref)


def select_step(routes_ref, gain_ref, sel_ref, tail_ref):
    select_table([routes_ref[:, k, :] for k in range(CAP)], sel_ref)
    tail_kernel(gain_ref, tail_ref)


def passed(piece, d, axis):
    n = lax.axis_size(axis)
    return lax.ppermute(piece, axis, [(i, (i + d) % n) for i in range(n)])


def select_kernel(recv_ref, sel_ref, tail_ref, out_ref):
    recv = recv_ref[...]
    for q in range(CAP):
        picked = dot(sel_ref[q], recv).astype(BF)
        for e in range(GROUP):
            out_ref[e, q * 16 : (q + 1) * 16, :] = picked[e * 16 : (e + 1) * 16]
    tail = tail_ref[...]
    for e in range(GROUP):
        out_ref[e, 64:72, :] = tail


def gate_up_kernel(rows_ref, *refs):
    *weights, out_ref = refs
    n = len(weights)
    x = lax.axis_index("x")
    squares = jnp.zeros((LANES, 1), F32)
    hidden = weights[0].shape[2]
    gate = jnp.zeros((LANES, hidden), F32)
    up = jnp.zeros((LANES, hidden), F32)
    for d in range(n):
        at = place_of(x - d + n, "x")
        raw = jnp.concatenate([rows_ref[at, 0:64, :], rows_ref[n + at, 0:64, :]], axis=0)
        raw = raw.astype(F32)
        tail = rows_ref[at, 64:72, :].astype(F32)
        gain = tail[0:1] + tail[1:2] + tail[2:3]
        squares = squares + jnp.sum(raw * raw, axis=1, keepdims=True)
        lhs = (raw * gain).astype(BF)
        gate = gate + dot(lhs, weights[d][0])
        up = up + dot(lhs, weights[d][1])
    ys = out_ref.shape[0]
    share, blocks = LANES // ys, hidden // LANES
    for i, total in enumerate((gate, up)):
        total = total.astype(BF)
        for j in range(blocks):
            part = total[:, j * LANES : (j + 1) * LANES]
            at = (i * blocks + j) * share
            for y in range(ys):
                out_ref[y, at : at + share, :] = part[y * share : (y + 1) * share]
    high = squares.astype(BF).astype(F32)
    low = squares - high
    lane = iota((8, LANES), 1)
    for y in range(ys):
        start = y * share
        first, second = slice(start, start + 8), slice(start + 8, start + 16)
        out_ref[y, 2 * blocks * share :, :] = jnp.where(
            lane < 32,
            high[first],
            jnp.where(lane < 64, low[first], jnp.where(lane < 96, high[second], low[second])),
        ).astype(BF)


def act_kernel(width, parts_ref, out_ref):
    ys, rows, _ = parts_ref.shape
    total = parts_ref[0].astype(F32)
    for y in range(1, ys):
        total = total + parts_ref[y].astype(F32)
    share = out_ref.shape[1] // ((rows - 8) // (2 * 16))
    tail = total[rows - 8 :]
    squares = jnp.concatenate(
        [tail[:, 0:1] + tail[:, 32:33], tail[:, 64:65] + tail[:, 96:97]], axis=0
    )
    scale = lax.rsqrt(squares / width + EPS)
    half = (rows - 8) // 2
    for j in range(half // share):
        gate = total[j * share : (j + 1) * share] * scale
        up = total[half + j * share : half + (j + 1) * share] * scale
        act = (gate / (1.0 + jnp.exp(-gate)) * up).astype(BF)
        for y in range(ys):
            out_ref[y, j * share : (j + 1) * share, :] = act


def slot_rows(act_ref):
    ys, rows, _ = act_ref.shape
    share = LANES // ys
    at = [GATHER.index(y) for y in REDUCE]
    return jnp.concatenate(
        [
            jnp.concatenate([act_ref[i, j : j + share, :] for i in at], axis=0)
            for j in range(0, rows, share)
        ],
        axis=1,
    )


def own_down_kernel(act_ref, scale_ref, weight_ref, out_ref):
    out_ref[...] = (dot(slot_rows(act_ref), weight_ref[0]) * scale_ref[...]).astype(BF)


def down_kernel(act_ref, scale_ref, own_ref, *refs):
    *weights, out_ref = refs
    n = len(weights) + 1
    x = lax.axis_index("x")
    act = slot_rows(act_ref)
    scale = scale_ref[...]
    for d in range(n):
        at = place_of(x - d + n, "x")
        out = (dot(act, weights[d - 1][0]) * scale).astype(BF) if d else own_ref[...]
        out_ref[at] = out[0:64]
        out_ref[n + at] = out[64:128]


def combine_kernel(parts_ref, sel_ref, out_ref):
    total = jnp.zeros((LANES, LANES), F32)
    for q in range(CAP):
        rows = jnp.concatenate(
            [parts_ref[e, q * 16 : (q + 1) * 16, :] for e in range(GROUP)], axis=0
        )
        total = total + dot_rows(sel_ref[q], rows)
    out_ref[...] = turned(total, lax.axis_size("z"), BACK).astype(BF)


def place_kernel(ret_ref, place_ref, comb_ref, squares_ref):
    chips = lax.axis_size("z")
    back = turned(ret_ref[...], chips, 2 * FIRST["z"](chips) - BACK)
    full = dot_rows(place_ref[...], back)
    comb_ref[...] = full[0:HALF] + full[HALF:LANES]
    squares = jnp.sum(full * full, axis=1, keepdims=True)
    flat = jnp.transpose(jnp.broadcast_to(squares, (LANES, LANES)))[0:1, :]
    for i in range(squares_ref.shape[0]):
        squares_ref[i] = flat


def norm_kernel(width, squares_ref, comb_ref, gain_ref, out_ref):
    total = squares_ref[0]
    for i in range(1, squares_ref.shape[0]):
        total = total + squares_ref[i]
    column = jnp.transpose(jnp.broadcast_to(total, (LANES, LANES)))
    column = column[0:HALF] + column[HALF:LANES]
    out_ref[...] = (comb_ref[...] * lax.rsqrt(column / width + EPS) * gain_ref[0:1, :]).astype(BF)


def listed(axes):
    order = [0]
    for axis in axes:
        n = lax.axis_size(axis)
        order = [i * n + (FIRST[axis](n) + STEP[axis] * k) % n for i in order for k in range(n)]
    return order


def exchange(value, axes, order=None):
    groups = [listed(axes) if order is None else order]
    return lax.all_to_all(value, axes, 0, 0, tiled=True, axis_index_groups=groups)


def on_device(tokens, in_gain, out_gain, routes, route_weights, w_gate, w_up, w_down):
    chips, ys, xs = lax.axis_size("z"), lax.axis_size("y"), lax.axis_size("x")
    local = tokens.shape[1]
    width = float(local * ys * xs)
    hidden = w_gate.shape[2]
    routes = jnp.transpose(routes.reshape(chips, LANES, CAP), (0, 2, 1))
    weights = jnp.transpose(route_weights.reshape(chips, LANES, CAP), (0, 2, 1))

    square = shape((LANES, LANES), BF)
    near, far, back, outgoing, place = deal(
        [w_gate, w_up], [1, 2, 3], (dispatch_step,), (routes, tokens), (square, square), out=(1,)
    )
    own, sel, tail = deal(
        [w_gate, w_up],
        [0],
        (select_step,),
        (routes, in_gain.reshape(1, local)),
        (shape((CAP, LANES, LANES), BF), shape((8, LANES), BF)),
    )
    gate_up = [own, passed(near, 1, "x"), passed(far, 2, "x"), passed(back, 3, "x")]
    own, near, far, back = deal([w_down], [0, 1, 2, 3])
    down = [own, passed(near, 1, "x"), passed(far, 2, "x"), passed(back, 3, "x")]
    arrived = exchange(outgoing.reshape(chips, GROUP, local), ("z",))
    slots = call(
        select_kernel, shape((GROUP, 72, LANES), BF), arrived.reshape(LANES, local), sel, tail
    )
    slots = exchange(slots, ("c", "x"))
    share = LANES // ys
    parts = call(
        gate_up_kernel, shape((ys, 2 * hidden // LANES * share + 8, LANES), BF), slots, *gate_up
    )
    scale, last_gain = call(
        scale_kernel,
        [shape((LANES, LANES), F32), shape((8, LANES), F32)],
        routes,
        weights,
        out_gain.reshape(1, local),
    )
    parts = exchange(parts, ("y",), REDUCE)
    act = call(
        lambda *refs: act_kernel(width, *refs),
        shape((ys, hidden // LANES * share, LANES), BF),
        parts,
    )
    act = exchange(act, ("y",), GATHER)
    own, *others = down
    own = call(own_down_kernel, shape((LANES, LANES), BF), act, scale, own)
    answers = call(down_kernel, shape((GROUP, 64, LANES), BF), act, scale, own, *others)
    answers = exchange(answers, ("c", "x"))
    mixed = call(combine_kernel, shape((LANES, local), BF), answers, sel)
    order = [(BACK + i) % chips for i in range(chips)]
    returned = exchange(mixed.reshape(chips, GROUP, local), ("z",), order)
    combined, squares = call(
        place_kernel,
        [shape((HALF, local), F32), shape((ys * xs, 1, LANES), F32)],
        returned.reshape(LANES, local),
        place,
    )
    squares = exchange(squares, ("y", "x"))
    return call(
        lambda *refs: norm_kernel(width, *refs),
        shape((HALF, local), BF),
        squares,
        combined,
        last_gain,
    )


def solution(mesh):
    fine = Mesh(
        mesh.devices.reshape(mesh.shape["ep"] // 2, 2, mesh.shape["tp"] // 4, 4),
        ("z", "c", "y", "x"),
    )
    ep, tp = ("z", "c"), ("y", "x")
    placed = (
        P(ep, tp),
        P(tp),
        P(tp),
        P(),
        P(),
        P(ep, tp, None),
        P(ep, tp, None),
        P(ep, None, tp),
    )

    return jax.shard_map(on_device, mesh=fine, in_specs=placed, out_specs=P(ep, tp), check_vma=False)
```

```python
import jax
import jax.numpy as jnp
from jax import lax
from jax.experimental import pallas as pl
from jax.experimental.pallas import tpu as pltpu
from jax.sharding import Mesh, PartitionSpec as P

EPS = 1e-06
BF, F32 = jnp.bfloat16, jnp.float32
LANES = 128
HALF = 64
CAP = 4
GROUP = 8
PARAMS = pltpu.CompilerParams(vmem_limit_bytes=16 * 1024 * 1024)
FIRST = {"z": lambda n: 14, "c": lambda n: n - 1, "y": lambda n: n // 2, "x": lambda n: n // 2}
STEP = {"z": 1, "c": 1, "y": 1, "x": 1}
BACK = 8
REDUCE = [4, 7, 2, 5, 0, 3, 6, 1]
GATHER = [4, 7, 2, 5, 0, 3, 6, 1]
VMEM = pl.BlockSpec(memory_space=pltpu.VMEM)
HBM = pl.BlockSpec(memory_space=pltpu.HBM)


def in_hbm(value):
    return pltpu.with_memory_space_constraint(value, pltpu.HBM)


def shape(dims, dtype):
    return jax.ShapeDtypeStruct(dims, dtype)


def iota(dims, dim):
    return lax.broadcasted_iota(jnp.int32, dims, dim)


def ones_where(mask, dtype=BF):
    return jnp.where(mask, 1.0, 0.0).astype(dtype)


def earlier():
    s, t = iota((LANES, LANES), 0), iota((LANES, LANES), 1)
    return ones_where((s < t) & ((s >> 6) == (t >> 6)))


def dot(a, b):
    return jnp.dot(a, b, preferred_element_type=F32)


def dot_rows(a, b):
    return lax.dot_general(a, b, (((0,), (0,)), ((), ())), preferred_element_type=F32)


def call(kernel, outs, *args):
    single = not isinstance(outs, (list, tuple))
    return pl.pallas_call(
        kernel,
        out_shape=outs,
        in_specs=[VMEM] * len(args),
        out_specs=VMEM if single else [VMEM] * len(outs),
        compiler_params=PARAMS,
    )(*args)


def turned(rows, chips, first):
    at = (first - FIRST["z"](chips)) % chips * (rows.shape[0] // chips)
    return jnp.concatenate([rows[at:], rows[:at]], axis=0) if at else rows


def place_of(index, axis):
    n = lax.axis_size(axis)
    return lax.rem(index + n - FIRST[axis](n), n)


def named(ids, expert):
    hit = ids[0] == expert
    for k in range(1, CAP):
        hit = hit | (ids[k] == expert)
    return jnp.where(hit, 1.0, 0.0)


def slice_copies(sources, outs, shifts, sems):
    x = lax.axis_index("x")
    return [
        pltpu.make_async_copy(
            source.at[lax.rem(x + d, source.shape[0])],
            out.at[i],
            sems.at[j * len(sources) + i],
        )
        for j, (d, out) in enumerate(zip(shifts, outs))
        for i, source in enumerate(sources)
    ]


def deal(arrays, shifts, kernels=(), extra=(), extra_outs=(), out=()):
    one = shape((len(arrays), *arrays[0].shape[1:]), BF)
    n, m, k = len(arrays), len(shifts), len(extra)
    through = [shifts.index(d) for d in out] + ([m] if out else [])
    shapes = [one] * m + list(extra_outs)

    def body(*refs):
        sources, small, rest = refs[:n], refs[n : n + k], refs[n + k :]
        outs, rest = list(rest[: len(shapes)]), rest[len(shapes) :]
        held, kept, (sems, small_sems, out_sems) = rest[:k], rest[k:-3], rest[-3:]
        stores = []
        for i, at in enumerate(through):
            stores.append(pltpu.make_async_copy(kept[i], outs[at], out_sems.at[i]))
            outs[at] = kept[i]
        fetches = [
            pltpu.make_async_copy(small[i], held[i], small_sems.at[i]) for i in range(k)
        ]
        copies = slice_copies(sources, outs[:m], shifts, sems)
        ahead = sorted(range(m * n), key=lambda i: i // n not in through)
        for copy in fetches + [copies[i] for i in ahead]:
            copy.start()
        for copy in fetches:
            copy.wait()
        for i, step in enumerate(kernels):
            step(*held, *outs[m:])
            if i == 0:
                for store, at in reversed(list(zip(stores, through))):
                    for copy in copies[at * n : (at + 1) * n]:
                        copy.wait()
                    store.start()
        for i, copy in enumerate(copies):
            if i // n not in through:
                copy.wait()
        for store in stores:
            store.wait()

    return pl.pallas_call(
        body,
        out_shape=shapes,
        in_specs=[HBM] * (n + k),
        out_specs=[HBM if i in through else VMEM for i in range(len(shapes))],
        scratch_shapes=[pltpu.VMEM(a.shape, a.dtype) for a in extra]
        + [pltpu.VMEM(shapes[i].shape, BF) for i in through]
        + [
            pltpu.SemaphoreType.DMA((m * n,)),
            pltpu.SemaphoreType.DMA((max(k, 1),)),
            pltpu.SemaphoreType.DMA((max(len(through), 1),)),
        ],
        compiler_params=PARAMS,
    )(*[in_hbm(a) for a in (*arrays, *extra)])


def dispatch(ids, tok_ref, out_ref, place_ref):
    z, c = lax.axis_index("z"), lax.axis_index("c")
    chips = ids[0].shape[0]
    first = jnp.sum(jnp.where(iota(ids[0].shape, 0) == z, ids[0], 0), axis=0, keepdims=True)
    group = first >> 3
    member = iota((chips, LANES), 0) == group
    rank = dot(ones_where(member), earlier())
    rank = jnp.sum(jnp.where(member, rank, 0.0), axis=0, keepdims=True).astype(jnp.int32)
    mine = (iota((1, LANES), 1) >> 6) == c
    row = jnp.where(mine, place_of(group, "z") * GROUP + rank, -1)
    place = ones_where(iota((LANES, LANES), 0) == row)
    place_ref[...] = place
    tok = tok_ref[...]
    out_ref[...] = dot(place, jnp.concatenate([tok, tok], axis=0)).astype(BF)


def select_table(ids, sel_ref):
    z, c = lax.axis_index("z"), lax.axis_index("c")
    chips = ids[0].shape[0]
    before = earlier()
    rows = [named(ids, z * GROUP + e) for e in listed(("c", "x"))]
    hits = jnp.concatenate(rows, axis=0)
    anyone = rows[0]
    for e in range(1, GROUP):
        anyone = jnp.maximum(anyone, rows[e])
    rank = dot(hits.astype(BF), before)
    start = (place_of(iota((chips, LANES), 0), "z") * GROUP).astype(F32)
    spot = dot(anyone.astype(BF), before) + start
    spots = jnp.concatenate([spot] * GROUP, axis=0)
    lane = iota((LANES, LANES), 1).astype(F32)
    live = (hits > 0.0) & ((iota((LANES, LANES), 1) >> 6) == c)
    for q in range(CAP):
        at = jnp.sum(jnp.where(live & (rank == q), spots + 1.0, 0.0), axis=1, keepdims=True) - 1.0
        sel_ref[q] = ones_where(lane == at)


def scale_kernel(routes_ref, weights_ref, gain_ref, scale_ref, last_ref):
    z, c, x = lax.axis_index("z"), lax.axis_index("c"), lax.axis_index("x")
    chips = routes_ref.shape[0]
    ids = [routes_ref[:, k, :] for k in range(CAP)]
    own = z * GROUP + c * CAP + x
    hit = named(ids, own)
    rank = dot(hit.astype(BF), earlier())
    weight = jnp.zeros((chips, LANES), F32)
    for k in range(CAP):
        weight = weight + jnp.where(ids[k] == own, weights_ref[:, k, :], 0.0)
    block = iota((chips, LANES), 1) >> 6
    for i, core in enumerate(listed(("c",))):
        for q in range(CAP):
            at = (hit > 0.0) & (rank == q) & (block == core)
            value = jnp.sum(jnp.where(at, weight, 0.0), axis=1, keepdims=True)
            start = (i * CAP + q) * chips
            scale_ref[start : start + chips, :] = jnp.broadcast_to(value, (chips, LANES))
    last_ref[...] = jnp.broadcast_to(gain_ref[...], last_ref.shape)


def tail_kernel(gain_ref, tail_ref):
    gain = gain_ref[...]
    high = gain.astype(BF).astype(F32)
    middle = (gain - high).astype(BF).astype(F32)
    low = gain - high - middle
    row = iota((8, LANES), 0)
    tail = jnp.where(row == 0, high, jnp.where(row == 1, middle, jnp.where(row == 2, low, 0.0)))
    tail_ref[...] = tail.astype(BF)


def dispatch_step(routes_ref, tok_ref, out_ref, place_ref):
    dispatch([routes_ref[:, k, :] for k in range(CAP)], tok_ref, out_ref, place_ref)


def select_step(routes_ref, gain_ref, sel_ref, tail_ref):
    select_table([routes_ref[:, k, :] for k in range(CAP)], sel_ref)
    tail_kernel(gain_ref, tail_ref)


def tail_copy(in_ref, out_ref):
    out_ref[...] = in_ref[...]


def passed(piece, d, axis):
    n = lax.axis_size(axis)
    return lax.ppermute(piece, axis, [(i, (i + d) % n) for i in range(n)])


def select_kernel(recv_ref, sel_ref, tail_ref, out_ref):
    recv = recv_ref[...]
    for q in range(CAP):
        picked = dot(sel_ref[q], recv).astype(BF)
        for e in range(GROUP):
            out_ref[e, q * 16 : (q + 1) * 16, :] = picked[e * 16 : (e + 1) * 16]
    tail = tail_ref[...]
    for e in range(GROUP):
        out_ref[e, 64:72, :] = tail


def gate_up_kernel(rows_ref, *refs):
    *weights, out_ref = refs
    n = len(weights)
    x = lax.axis_index("x")
    squares = jnp.zeros((LANES, 1), F32)
    hidden = weights[0].shape[2]
    gate = jnp.zeros((LANES, hidden), F32)
    up = jnp.zeros((LANES, hidden), F32)
    for d in range(n):
        at = place_of(x - d + n, "x")
        raw = jnp.concatenate([rows_ref[at, 0:64, :], rows_ref[n + at, 0:64, :]], axis=0)
        raw = raw.astype(F32)
        tail = rows_ref[at, 64:72, :].astype(F32)
        gain = tail[0:1] + tail[1:2] + tail[2:3]
        squares = squares + jnp.sum(raw * raw, axis=1, keepdims=True)
        lhs = (raw * gain).astype(BF)
        gate = gate + dot(lhs, weights[d][0])
        up = up + dot(lhs, weights[d][1])
    ys = out_ref.shape[0]
    share, blocks = LANES // ys, hidden // LANES
    for i, total in enumerate((gate, up)):
        total = total.astype(BF)
        for j in range(blocks):
            part = total[:, j * LANES : (j + 1) * LANES]
            at = (i * blocks + j) * share
            for y in range(ys):
                out_ref[y, at : at + share, :] = part[y * share : (y + 1) * share]
    high = squares.astype(BF).astype(F32)
    low = squares - high
    lane = iota((8, LANES), 1)
    for y in range(ys):
        start = y * share
        first, second = slice(start, start + 8), slice(start + 8, start + 16)
        out_ref[y, 2 * blocks * share :, :] = jnp.where(
            lane < 32,
            high[first],
            jnp.where(lane < 64, low[first], jnp.where(lane < 96, high[second], low[second])),
        ).astype(BF)


def act_kernel(width, parts_ref, out_ref):
    ys, rows, _ = parts_ref.shape
    total = parts_ref[0].astype(F32)
    for y in range(1, ys):
        total = total + parts_ref[y].astype(F32)
    share = out_ref.shape[1] // ((rows - 8) // (2 * 16))
    tail = total[rows - 8 :]
    squares = jnp.concatenate(
        [tail[:, 0:1] + tail[:, 32:33], tail[:, 64:65] + tail[:, 96:97]], axis=0
    )
    scale = lax.rsqrt(squares / width + EPS)
    half = (rows - 8) // 2
    for j in range(half // share):
        gate = total[j * share : (j + 1) * share] * scale
        up = total[half + j * share : half + (j + 1) * share] * scale
        act = (gate / (1.0 + jnp.exp(-gate)) * up).astype(BF)
        for y in range(ys):
            out_ref[y, j * share : (j + 1) * share, :] = act


def slot_rows(act_ref):
    ys, rows, _ = act_ref.shape
    share = LANES // ys
    at = [GATHER.index(y) for y in REDUCE]
    return jnp.concatenate(
        [
            jnp.concatenate([act_ref[i, j : j + share, :] for i in at], axis=0)
            for j in range(0, rows, share)
        ],
        axis=1,
    )


def own_down_kernel(act_ref, scale_ref, weight_ref, out_ref):
    out_ref[...] = (dot(slot_rows(act_ref), weight_ref[0]) * scale_ref[...]).astype(BF)


def down_kernel(act_ref, scale_ref, own_ref, *refs):
    *weights, out_ref = refs
    n = len(weights) + 1
    x = lax.axis_index("x")
    act = slot_rows(act_ref)
    scale = scale_ref[...]
    for d in range(n):
        at = place_of(x - d + n, "x")
        out = (dot(act, weights[d - 1][0]) * scale).astype(BF) if d else own_ref[...]
        out_ref[at] = out[0:64]
        out_ref[n + at] = out[64:128]


def combine_kernel(parts_ref, sel_ref, out_ref):
    total = jnp.zeros((LANES, LANES), F32)
    for q in range(CAP):
        rows = jnp.concatenate(
            [parts_ref[e, q * 16 : (q + 1) * 16, :] for e in range(GROUP)], axis=0
        )
        total = total + dot_rows(sel_ref[q], rows)
    out_ref[...] = turned(total, lax.axis_size("z"), BACK).astype(BF)


def place_kernel(ret_ref, place_ref, comb_ref, squares_ref):
    chips = lax.axis_size("z")
    back = turned(ret_ref[...], chips, 2 * FIRST["z"](chips) - BACK)
    full = dot_rows(place_ref[...], back)
    comb_ref[...] = full[0:HALF] + full[HALF:LANES]
    squares = jnp.sum(full * full, axis=1, keepdims=True)
    flat = jnp.transpose(jnp.broadcast_to(squares, (LANES, LANES)))[0:1, :]
    for i in range(squares_ref.shape[0]):
        squares_ref[i] = flat


def norm_kernel(width, squares_ref, comb_ref, gain_ref, out_ref):
    total = squares_ref[0]
    for i in range(1, squares_ref.shape[0]):
        total = total + squares_ref[i]
    column = jnp.transpose(jnp.broadcast_to(total, (LANES, LANES)))
    column = column[0:HALF] + column[HALF:LANES]
    out_ref[...] = (comb_ref[...] * lax.rsqrt(column / width + EPS) * gain_ref[0:1, :]).astype(BF)


def listed(axes):
    order = [0]
    for axis in axes:
        n = lax.axis_size(axis)
        order = [i * n + (FIRST[axis](n) + STEP[axis] * k) % n for i in order for k in range(n)]
    return order


def exchange(value, axes, order=None):
    groups = [listed(axes) if order is None else order]
    return lax.all_to_all(value, axes, 0, 0, tiled=True, axis_index_groups=groups)


def on_device(tokens, in_gain, out_gain, routes, route_weights, w_gate, w_up, w_down):
    chips, ys, xs = lax.axis_size("z"), lax.axis_size("y"), lax.axis_size("x")
    local = tokens.shape[1]
    width = float(local * ys * xs)
    hidden = w_gate.shape[2]
    routes = jnp.transpose(routes.reshape(chips, LANES, CAP), (0, 2, 1))
    weights = jnp.transpose(route_weights.reshape(chips, LANES, CAP), (0, 2, 1))

    square = shape((LANES, LANES), BF)
    near, far, outgoing, place = deal(
        [w_gate, w_up], [1, 2], (dispatch_step,), (routes, tokens), (square, square), out=(1,)
    )
    own, back, sel, gains = deal(
        [w_gate, w_up],
        [0, 3],
        (select_step,),
        (routes, in_gain.reshape(1, local)),
        (shape((CAP, LANES, LANES), BF), shape((8, LANES), BF)),
    )
    tail = call(tail_copy, shape((8, LANES), BF), gains)
    gate_up = [own, passed(near, 1, "x"), passed(far, 2, "x"), passed(back, 3, "x")]
    own, near, far, back = deal([w_down], [0, 1, 2, 3])
    down = [own, passed(near, 1, "x"), passed(far, 2, "x"), passed(back, 3, "x")]
    arrived = exchange(outgoing.reshape(chips, GROUP, local), ("z",))
    slots = call(
        select_kernel, shape((GROUP, 72, LANES), BF), arrived.reshape(LANES, local), sel, tail
    )
    slots = exchange(slots, ("c", "x"))
    share = LANES // ys
    parts = call(
        gate_up_kernel, shape((ys, 2 * hidden // LANES * share + 8, LANES), BF), slots, *gate_up
    )
    scale, last_gain = call(
        scale_kernel,
        [shape((LANES, LANES), F32), shape((8, LANES), F32)],
        routes,
        weights,
        out_gain.reshape(1, local),
    )
    parts = exchange(parts, ("y",), REDUCE)
    act = call(
        lambda *refs: act_kernel(width, *refs),
        shape((ys, hidden // LANES * share, LANES), BF),
        parts,
    )
    act = exchange(act, ("y",), GATHER)
    own, *others = down
    own = call(own_down_kernel, shape((LANES, LANES), BF), act, scale, own)
    answers = call(down_kernel, shape((GROUP, 64, LANES), BF), act, scale, own, *others)
    answers = exchange(answers, ("c", "x"))
    mixed = call(combine_kernel, shape((LANES, local), BF), answers, sel)
    order = [(BACK + i) % chips for i in range(chips)]
    returned = exchange(mixed.reshape(chips, GROUP, local), ("z",), order)
    combined, squares = call(
        place_kernel,
        [shape((HALF, local), F32), shape((ys * xs, 1, LANES), F32)],
        returned.reshape(LANES, local),
        place,
    )
    squares = exchange(squares, ("y", "x"))
    return call(
        lambda *refs: norm_kernel(width, *refs),
        shape((HALF, local), BF),
        squares,
        combined,
        last_gain,
    )


def solution(mesh):
    fine = Mesh(
        mesh.devices.reshape(mesh.shape["ep"] // 2, 2, mesh.shape["tp"] // 4, 4),
        ("z", "c", "y", "x"),
    )
    ep, tp = ("z", "c"), ("y", "x")
    placed = (
        P(ep, tp),
        P(tp),
        P(tp),
        P(),
        P(),
        P(ep, tp, None),
        P(ep, tp, None),
        P(ep, None, tp),
    )

    return jax.shard_map(on_device, mesh=fine, in_specs=placed, out_specs=P(ep, tp), check_vma=False)
```
